128 devices in a mesh: ep: 128 (over z, y, x, core).
Axes of the slice: x: 4, y: 4, z: 4, core: 2. Of those that a mesh axis runs over, the one named last changes fastest.
Arguments:
- tokens: bfloat16 [6144, 2048], P('ep'), may hold values from -6 to 6
- history_length: int32 [6144], P('ep'), may hold values from 1024 to 8192
- norm_gain: float32 [2048], replicated, may hold values from 0.1 to 1.9
- w_query: bfloat16 [2048, 512], replicated, may hold values from -0.125 to 0.125
- w_key: bfloat16 [2048, 512], replicated, may hold values from -0.125 to 0.125
- w_value: bfloat16 [2048, 512], replicated, may hold values from -0.125 to 0.125
- w_gate: bfloat16 [2048, 512], replicated, may hold values from -0.125 to 0.125
- decay_rate: float32 [8], replicated, may hold values from 0.003 to 0.7
- state: float32 [6144, 8, 64, 64], P('ep'), may hold values from -4 to 4
- head_gain: float32 [512], replicated, may hold values from 0.1 to 1.9
- w_out: bfloat16 [512, 2048], replicated, may hold values from -0.25 to 0.25
- moe_gain: float32 [2048], replicated, may hold values from 0.1 to 1.9
- route_weights: float32 [6144, 2], P('ep'), may hold values from 0.3 to 3
- expert_group: int32 [6144], P('ep'), may hold values from 0 to 3, as said below
- expert_inner: int32 [6144, 2], P('ep'), may hold values from 0 to 31, as said below
- expert_gate: bfloat16 [128, 2048, 256], P('ep'), may hold values from -0.125 to 0.125
- expert_up: bfloat16 [128, 2048, 256], P('ep'), may hold values from -0.125 to 0.125
- expert_down: bfloat16 [128, 256, 2048], P('ep'), may hold values from -0.375 to 0.375
Outputs:
- output: bfloat16 [6144, 2048], P('ep')
- new_state: float32 [6144, 8, 64, 64], P('ep')
The draws below stay inside these ranges and needn't reach their ends.
Inputs may be any that keep to these rules, and one draw needn't show every extreme that they name: `expert_group`: together with expert_inner it names 2 different experts of one group for each token. `expert_inner`: the rows of one device name one expert at most 2 times; in every draw some expert is named exactly 2 times by the rows of every device.
All inputs are finite; a program needn't handle non-finite values.
Results may differ from the reference program's by a relative error of at most 0.02.
Values may be sent and summed in bfloat16 or wider, within the bound.
A program may use at most 128 MiB of HBM per device.

```python
import math
import jax
import jax.numpy as jnp
from jax import lax

D = 2048
HEADS = 8
HEAD_DIM = 64
RET_WIDTH = 512
EXPERT_WIDTH = 256
SEQ_DEV = 48
TOKENS = 6144
EXPERTS = 128
GROUPS = 4
GROUP_SIZE = 32
TOP_K = 2
CAP = 2
N_EP = 128


def route_table(key):
    root_key = jax.random.fold_in(key, 7)
    pair_count = EXPERTS * CAP // 2
    per_group = pair_count // GROUPS
    hot_group = jax.random.randint(jax.random.fold_in(root_key, 1), (), 0, GROUPS)
    relabel = jax.vmap(lambda subkey: jax.random.permutation(subkey, GROUP_SIZE))(jax.random.split(jax.random.fold_in(root_key, 2), GROUPS))
    pair_ids = jnp.arange(pair_count, dtype=jnp.int32)
    pair_group = pair_ids // per_group
    pair_offset = pair_ids % per_group
    first_inner = relabel[pair_group, 2 * pair_offset % GROUP_SIZE]
    second_inner = relabel[pair_group, (2 * pair_offset + 1) % GROUP_SIZE]
    heated = (pair_group == hot_group) & (pair_offset % (GROUP_SIZE // 2) == 0)

    def one_block(subkey):
        jitter = jax.random.randint(jax.random.fold_in(subkey, 1), (pair_count,), 0, 1 << 20)
        scores = jnp.where(heated, pair_ids, (jitter + 1) * pair_count + pair_ids)
        _, chosen = lax.top_k(-scores, SEQ_DEV)
        chosen = chosen[jax.random.permutation(jax.random.fold_in(subkey, 2), SEQ_DEV)]
        return (pair_group[chosen], jnp.stack([first_inner[chosen], second_inner[chosen]], axis=-1))
    groups, inner_ids = jax.vmap(one_block)(jax.random.split(jax.random.fold_in(root_key, 3), TOKENS // SEQ_DEV))
    return (groups.reshape(TOKENS).astype(jnp.int32), inner_ids.reshape(TOKENS, TOP_K).astype(jnp.int32))


def draw_expert_group(key, part):
    return route_table(key)[0]


def draw_expert_inner(key, part):
    return route_table(key)[1]


def place_ends(result, own_key, least, largest):
    dims = result.shape
    index_at = [jax.random.randint(jax.random.fold_in(own_key, axis), (), 0, dims[axis]) for axis in range(len(dims))]
    result = result.at[tuple(index_at)].set(least)
    longest = dims.index(max(dims))
    index_at[longest] = (index_at[longest] + 1) % dims[longest]
    return result.at[tuple(index_at)].set(largest)


def block_levels(own_key, extent, cuts, low, high):
    level = 1.0
    for position, shards_of in cuts:
        steps = jax.random.uniform(jax.random.fold_in(jax.random.fold_in(own_key, 6), position), (shards_of,), jnp.float32, low / len(cuts), high / len(cuts))
        level = level * jnp.repeat(jnp.exp(steps), extent[position] // shards_of).reshape((-1,) + (1,) * (len(extent) - 1 - position))
    return level


def normal_values(own_key, extent, scale, most, cuts=(), held_as=jnp.bfloat16):
    values = scale * jax.random.normal(own_key, extent, jnp.float32)
    if cuts:
        values = values * block_levels(own_key, extent, cuts, -0.22, 0.18)
    return jnp.clip(values, -most, most).astype(held_as)


def setup_inputs(seed: int = 0) -> dict:
    key_list = jax.random.split(jax.random.key(seed), 19)
    return {
        "tokens": normal_values(key_list[0], (TOKENS, D), 1.0, 6.0, ((0, 128),)),
        "history_length": place_ends(jax.random.randint(key_list[1], (TOKENS,), 1024, 8193), jax.random.fold_in(key_list[1], 1), 1024, 8192).astype(jnp.int32),
        "norm_gain": jnp.clip(1.0 + 0.18 * jax.random.normal(key_list[2], (D,), jnp.float32), 0.1, 1.9),
        "w_query": normal_values(key_list[3], (D, RET_WIDTH), D ** -0.5, 0.125),
        "w_key": normal_values(key_list[4], (D, RET_WIDTH), D ** -0.5, 0.125),
        "w_value": normal_values(key_list[5], (D, RET_WIDTH), D ** -0.5, 0.125),
        "w_gate": normal_values(key_list[6], (D, RET_WIDTH), D ** -0.5, 0.125),
        "decay_rate": jnp.clip(jnp.exp(jax.random.uniform(key_list[7], (HEADS,), jnp.float32, math.log(0.003), math.log(0.7))), 0.003, 0.7),
        "state": normal_values(key_list[8], (TOKENS, HEADS, HEAD_DIM, HEAD_DIM), 0.3, 4.0, ((0, 128),), jnp.float32),
        "head_gain": jnp.clip(1.0 + 0.18 * jax.random.normal(key_list[9], (RET_WIDTH,), jnp.float32), 0.1, 1.9),
        "w_out": normal_values(key_list[10], (RET_WIDTH, D), RET_WIDTH ** -0.5, 0.25),
        "moe_gain": jnp.clip(1.0 + 0.18 * jax.random.normal(key_list[11], (D,), jnp.float32), 0.1, 1.9),
        "route_weights": jnp.clip(jnp.exp(math.log(3.0) - 2.3025851 * jax.random.uniform(key_list[12], (TOKENS, TOP_K), jnp.float32) ** block_levels(key_list[12], (TOKENS, TOP_K), ((0, 128),), -0.2, 0.2)), 0.3, 3.0),
        "expert_group": draw_expert_group(jax.random.fold_in(key_list[18], 71), 0),
        "expert_inner": draw_expert_inner(jax.random.fold_in(key_list[18], 71), 0),
        "expert_gate": normal_values(key_list[15], (EXPERTS, D, EXPERT_WIDTH), D ** -0.5, 0.125, ((0, 128),)),
        "expert_up": normal_values(key_list[16], (EXPERTS, D, EXPERT_WIDTH), D ** -0.5, 0.125, ((0, 128),)),
        "expert_down": normal_values(key_list[17], (EXPERTS, EXPERT_WIDTH, D), EXPERT_WIDTH ** -0.5, 0.375, ((0, 128),)),
    }


epsilon = 1e-06

def rotate(values, places):
    halfway = values.shape[-1] // 2
    inverse = 10000.0 ** (-jnp.arange(halfway, dtype=jnp.float32) / halfway)
    angles = places[:, None] * inverse[None, :]
    cosine = jnp.cos(angles)[:, None, :]
    sine_table = jnp.sin(angles)[:, None, :]
    first_half = values[..., :halfway]
    second = values[..., halfway:]
    return jnp.concatenate([first_half * cosine - second * sine_table, first_half * sine_table + second * cosine], axis=-1)

def rms_scale(values, gains):
    return values * lax.rsqrt(lax.optimization_barrier(jnp.mean(values * values, axis=-1, keepdims=True)) + epsilon) * gains

def retention_step(tokens, history_length, norm_gain, w_query, w_key, w_value, w_gate, decay_rate, state, head_gain, w_out, moe_gain):
    row_count = tokens.shape[0]
    head_count = decay_rate.shape[0]
    head_width = state.shape[-1]
    inputs = tokens.astype(jnp.float32)
    normed = rms_scale(inputs, norm_gain).astype(jnp.bfloat16)

    def project(weights):
        return jnp.dot(normed, weights, preferred_element_type=jnp.float32).astype(jnp.bfloat16)
    queries = project(w_query).reshape(row_count, head_count, head_width).astype(jnp.float32)
    keys_now = project(w_key).reshape(row_count, head_count, head_width).astype(jnp.float32)
    values_now = project(w_value).reshape(row_count, head_count, head_width).astype(jnp.float32)
    gating = project(w_gate).astype(jnp.float32)
    places = history_length.astype(jnp.float32)
    queries = rotate(queries, places)
    keys_now = rotate(keys_now, places) * head_width ** (-0.5)
    retain = jnp.exp(-decay_rate)
    new_state = retain[None, :, None, None] * state + keys_now[:, :, :, None] * values_now[:, :, None, :]
    reading = jnp.einsum('bhk,bhkv->bhv', queries, new_state, precision=lax.Precision.HIGHEST)
    reading = rms_scale(reading, head_gain.reshape(head_count, head_width))
    mixed_heads = (reading.reshape(row_count, head_count * head_width) * jax.nn.silu(gating)).astype(jnp.bfloat16)
    mixed_tokens = (inputs + jnp.dot(mixed_heads, w_out, preferred_element_type=jnp.float32)).astype(jnp.bfloat16)
    normed_moe = rms_scale(mixed_tokens.astype(jnp.float32), moe_gain).astype(jnp.bfloat16)
    return (mixed_tokens, normed_moe, new_state)

def expert_apply(row_block, gate_weight, up_weight, down_weight):
    gate_part = jnp.dot(row_block, gate_weight, preferred_element_type=jnp.float32)
    up_part = jnp.dot(row_block, up_weight, preferred_element_type=jnp.float32)
    hidden = (jax.nn.silu(gate_part) * up_part).astype(jnp.bfloat16)
    return jnp.dot(hidden, down_weight, preferred_element_type=jnp.float32).astype(jnp.bfloat16)

def reference(tokens, history_length, norm_gain, w_query, w_key, w_value, w_gate, decay_rate, state, head_gain, w_out, moe_gain, route_weights, expert_group, expert_inner, expert_gate, expert_up, expert_down):
    mixed_tokens, normed_moe, new_state = retention_step(tokens, history_length, norm_gain, w_query, w_key, w_value, w_gate, decay_rate, state, head_gain, w_out, moe_gain)
    row_count = tokens.shape[0]
    experts = expert_gate.shape[0]
    per_group = experts // GROUPS
    flat_ids = (expert_group[:, None] * per_group + expert_inner).reshape(-1).astype(jnp.int32)
    slot_total = flat_ids.shape[0]
    padded_ids = jnp.concatenate([flat_ids, jnp.full((1,), -1, jnp.int32)])
    owners = jnp.concatenate([jnp.arange(slot_total, dtype=jnp.int32) // TOP_K, jnp.zeros((1,), jnp.int32)])
    scales = jnp.concatenate([route_weights.reshape(-1), jnp.zeros((1,), jnp.float32)])
    row_bound = N_EP * CAP

    def visit_expert(running, expert):
        matched = padded_ids == expert
        picked = jnp.nonzero(matched, size=row_bound, fill_value=slot_total)[0].astype(jnp.int32)
        owner_rows = owners[picked]
        weighting = jnp.where(matched[picked], scales[picked], jnp.zeros_like(scales[picked]))
        outputs = expert_apply(normed_moe[owner_rows], expert_gate[expert], expert_up[expert], expert_down[expert])
        running = running.at[owner_rows].add(outputs.astype(jnp.float32) * weighting[:, None])
        return (running, None)
    running, _ = lax.scan(visit_expert, jnp.zeros((row_count, tokens.shape[1]), jnp.float32), jnp.arange(experts, dtype=jnp.int32))
    output = (mixed_tokens.astype(jnp.float32) + running).astype(jnp.bfloat16)
    return (output, new_state)
```

```python
import functools

import jax
import jax.numpy as jnp
from jax import lax
from jax.experimental import pallas as pl
from jax.experimental.pallas import tpu as pltpu
from jax.sharding import PartitionSpec as P

MESH = pl.DeviceIdType.MESH
F32 = jnp.float32
BF16 = jnp.bfloat16
GROUP_SIZE = 32
CHUNKS = 4
epsilon = 1e-06


def rotate(values, places):
    halfway = values.shape[-1] // 2
    inverse = 10000.0 ** (-jnp.arange(halfway, dtype=jnp.float32) / halfway)
    angles = places[:, None] * inverse[None, :]
    cosine = jnp.cos(angles)[:, None, :]
    sine_table = jnp.sin(angles)[:, None, :]
    first_half = values[..., :halfway]
    second = values[..., halfway:]
    return jnp.concatenate(
        [first_half * cosine - second * sine_table, first_half * sine_table + second * cosine],
        axis=-1,
    )


def rms_scale(values, gains):
    return values * lax.rsqrt(jnp.mean(values * values, axis=-1, keepdims=True) + epsilon) * gains


def retention_step(
    tokens, history_length, norm_gain, w_query, w_key, w_value, w_gate, decay_rate, state,
    head_gain, w_out, moe_gain,
):
    row_count = tokens.shape[0]
    head_count = decay_rate.shape[0]
    head_width = state.shape[-1]
    inputs = tokens.astype(jnp.float32)
    normed = rms_scale(inputs, norm_gain).astype(jnp.bfloat16)

    def project(weights):
        return jnp.dot(normed, weights, preferred_element_type=jnp.float32).astype(jnp.bfloat16)

    queries = project(w_query).reshape(row_count, head_count, head_width).astype(jnp.float32)
    keys_now = project(w_key).reshape(row_count, head_count, head_width).astype(jnp.float32)
    values_now = project(w_value).reshape(row_count, head_count, head_width).astype(jnp.float32)
    gating = project(w_gate).astype(jnp.float32)
    places = history_length.astype(jnp.float32)
    queries = rotate(queries, places)
    keys_now = rotate(keys_now, places) * head_width ** (-0.5)
    retain = jnp.exp(-decay_rate)
    new_state = (
        retain[None, :, None, None] * state + keys_now[:, :, :, None] * values_now[:, :, None, :]
    )
    reading = jnp.einsum("bhk,bhkv->bhv", queries, new_state)
    reading = rms_scale(reading, head_gain.reshape(head_count, head_width))
    mixed_heads = (
        reading.reshape(row_count, head_count * head_width) * jax.nn.silu(gating)
    ).astype(jnp.bfloat16)
    mixed_tokens = (
        inputs + jnp.dot(mixed_heads, w_out, preferred_element_type=jnp.float32)
    ).astype(jnp.bfloat16)
    normed_moe = rms_scale(mixed_tokens.astype(jnp.float32), moe_gain).astype(jnp.bfloat16)
    return (mixed_tokens, normed_moe, new_state)


def far_first(t):
    return (2 + 3 * ((t * (t + 1)) // 2)) % 4


def digits(me):
    return me // 32, (me // 8) % 4, (me // 2) % 4, me % 2


def partner(me, j, sign):
    z, y, x, c = digits(me)
    dz, dy, dx = far_first(j // 32), far_first((j // 8) % 4), far_first((j // 2) % 4)
    return (
        ((z + 4 + sign * dz) % 4) * 32
        + ((y + 4 + sign * dy) % 4) * 8
        + ((x + 4 + sign * dx) % 4) * 2
        + (c + 1 - j % 2) % 2
    )


def slot_experts(me, r):
    z, y, x, c = digits(me)
    j = r >> 1

    def far(t):
        return (2 + 3 * ((t * (t + 1)) >> 1)) & 3

    return (
        ((z + far(j >> 5)) & 3) * 32
        + ((y + far((j >> 3) & 3)) & 3) * 8
        + ((x + far((j >> 1) & 3)) & 3) * 2
        + ((c + 1 - (j & 1)) & 1)
    )


def moe_kernel(
    normed_ref, mixed_ref, group_ref, inner_ref, route_ref, gate_hbm, up_hbm, down_hbm, out_ref,
    gate_w, up_w, down_w, outgoing, incoming, results, returned,
    weight_sems, send_one, recv_one, send_two, recv_two,
):
    me = lax.axis_index("ep")
    rows = normed_ref.shape[0]
    n = outgoing.shape[0]
    slots = 2 * n
    per = n // CHUNKS
    loads = [
        pltpu.make_async_copy(src.at[0], dst, weight_sems.at[i])
        for i, (src, dst) in enumerate(((gate_hbm, gate_w), (up_hbm, up_w), (down_hbm, down_w)))
    ]
    for load in loads:
        load.start()
    barrier = pltpu.get_barrier_semaphore()

    def greet(j, carry):
        pl.semaphore_signal(barrier, inc=1, device_id=(partner(me, j, 1),), device_id_type=MESH)
        return carry

    lax.fori_loop(0, n - 1, greet, 0)

    first_row = group_ref[...] * GROUP_SIZE + inner_ref[0:1, :]
    second_row = group_ref[...] * GROUP_SIZE + inner_ref[1:2, :]
    sub = lax.broadcasted_iota(jnp.int32, (rows, rows), 0)
    lane = lax.broadcasted_iota(jnp.int32, (rows, rows), 1)

    def column(row):
        return jnp.sum(jnp.where(sub == lane, row, jnp.zeros_like(row)), axis=1, keepdims=True)

    first_col, second_col = column(first_row), column(second_row)

    def rank(ids_row):
        same = (first_col == ids_row).astype(F32) + (second_col == ids_row).astype(F32)
        return jnp.sum(jnp.where(sub < lane, same, 0.0), axis=0, keepdims=True)

    first_rank, second_rank = rank(first_row), rank(second_row)
    r_col = lax.broadcasted_iota(jnp.int32, (slots, 1), 0)
    expert_col = slot_experts(me, r_col)
    k_col = (r_col & 1).astype(F32)
    place = ((expert_col == first_row) & (k_col == first_rank)) | (
        (expert_col == second_row) & (k_col == second_rank)
    )
    place = place.astype(F32).astype(BF16)
    outgoing[...] = (
        jnp.dot(place, normed_ref[...], preferred_element_type=F32)
        .astype(BF16)
        .reshape(n, 2, normed_ref.shape[1])
    )
    pl.semaphore_wait(barrier, n - 1)

    def dispatch(j, carry):
        pltpu.make_async_remote_copy(
            src_ref=outgoing.at[j], dst_ref=incoming.at[j], send_sem=send_one,
            recv_sem=recv_one.at[j // per], device_id=(partner(me, j, 1),), device_id_type=MESH,
        ).start()
        return carry

    lax.fori_loop(0, n - 1, dispatch, 0)
    incoming[n - 1] = outgoing[n - 1]
    for load in loads:
        load.wait()

    def give_back(j, carry):
        pltpu.make_async_remote_copy(
            src_ref=results.at[j], dst_ref=returned.at[j], send_sem=send_two,
            recv_sem=recv_two.at[j // per], device_id=(partner(me, j, -1),), device_id_type=MESH,
        ).start()
        return carry

    def wait_block(ref, sem, start, count):
        block = ref.at[pl.ds(start, count)]
        pltpu.make_async_copy(block, block, sem).wait()

    for chunk in range(CHUNKS):
        start = chunk * per
        count = per if chunk < CHUNKS - 1 else per - 1
        wait_block(incoming, recv_one.at[chunk], start, count)
        x = incoming[pl.ds(start, per)].reshape(2 * per, incoming.shape[2])
        gate_part = jnp.dot(x, gate_w[...], preferred_element_type=F32)
        up_part = jnp.dot(x, up_w[...], preferred_element_type=F32)
        hidden = (gate_part * jax.nn.sigmoid(gate_part) * up_part).astype(BF16)
        y = jnp.dot(hidden, down_w[...], preferred_element_type=F32).astype(BF16)
        results[pl.ds(start, per)] = y.reshape(per, 2, y.shape[1])
        lax.fori_loop(start, start + count, give_back, 0)
    returned[n - 1] = results[n - 1]

    r_row = lax.broadcasted_iota(jnp.int32, (1, slots), 1)
    expert_row = slot_experts(me, r_row)
    k_row = (r_row & 1).astype(F32)
    route_one, route_two = column(route_ref[0:1, :]), column(route_ref[1:2, :])
    first_k, second_k = column(first_rank), column(second_rank)
    weights = jnp.where(
        (first_col == expert_row) & (first_k == k_row), route_one, 0.0
    ) + jnp.where((second_col == expert_row) & (second_k == k_row), route_two, 0.0)
    high = weights.astype(BF16)
    low = (weights - high.astype(F32)).astype(BF16)
    for chunk in range(CHUNKS):
        start = chunk * per
        count = per if chunk < CHUNKS - 1 else per - 1
        wait_block(returned, recv_two.at[chunk], start, count)
    back = returned[...].reshape(slots, returned.shape[2])
    routed = jnp.dot(high, back, preferred_element_type=F32) + jnp.dot(
        low, back, preferred_element_type=F32
    )
    out_ref[...] = (mixed_ref[...].astype(F32) + routed).astype(BF16)
    wait_block(outgoing, send_one, 0, n - 1)
    wait_block(results, send_two, 0, n - 1)


def local(
    tokens, history_length, norm_gain, w_query, w_key, w_value, w_gate, decay_rate, state,
    head_gain, w_out, moe_gain, route_weights, expert_group, expert_inner, expert_gate,
    expert_up, expert_down,
):
    experts = lax.axis_size("ep")
    rows, width = tokens.shape
    hidden = expert_gate.shape[2]
    mixed_tokens, normed_moe, new_state = retention_step(
        tokens, history_length, norm_gain, w_query, w_key, w_value, w_gate, decay_rate, state,
        head_gain, w_out, moe_gain,
    )
    vmem = pl.BlockSpec(memory_space=pltpu.VMEM)
    hbm = pl.BlockSpec(memory_space=pl.ANY)
    slab = pltpu.VMEM((experts, 2, width), BF16)
    output = pl.pallas_call(
        moe_kernel,
        out_shape=jax.ShapeDtypeStruct((rows, width), BF16),
        in_specs=[vmem] * 5 + [hbm] * 3,
        out_specs=vmem,
        scratch_shapes=[
            pltpu.VMEM((width, hidden), BF16),
            pltpu.VMEM((width, hidden), BF16),
            pltpu.VMEM((hidden, width), BF16),
            slab, slab, slab, slab,
            pltpu.SemaphoreType.DMA((3,)),
            pltpu.SemaphoreType.DMA,
            pltpu.SemaphoreType.DMA((CHUNKS,)),
            pltpu.SemaphoreType.DMA,
            pltpu.SemaphoreType.DMA((CHUNKS,)),
        ],
        compiler_params=pltpu.CompilerParams(
            collective_id=0, has_side_effects=True, vmem_limit_bytes=40 * 1024 * 1024
        ),
    )(
        normed_moe, mixed_tokens, expert_group.reshape(1, rows), expert_inner.T,
        route_weights.T, expert_gate, expert_up, expert_down,
    )
    return (output, new_state)


def solution(mesh):
    return jax.shard_map(
        local,
        mesh=mesh,
        in_specs=(
            P("ep", None), P("ep"), P(), P(), P(), P(), P(), P(), P("ep", None, None, None),
            P(), P(), P(), P("ep", None), P("ep"), P("ep", None), P("ep", None, None),
            P("ep", None, None), P("ep", None, None),
        ),
        out_specs=(P("ep", None), P("ep", None, None, None)),
        check_vma=False,
    )
```

```python
import numpy as np

import jax
import jax.numpy as jnp
from jax import lax
from jax.experimental import pallas as pl
from jax.experimental.pallas import tpu as pltpu
from jax.sharding import PartitionSpec as P

MESH = pl.DeviceIdType.MESH
F32 = jnp.float32
BF16 = jnp.bfloat16
GROUP_SIZE = 32
PLANES = 4
CHUNKS = 2
STATE_BLOCK = 8
epsilon = 1e-06


FAR = (2, 1, 3, 0)


def digits(me):
    return me // 32, (me // 8) % 4, (me // 2) % 4, me % 2


def each_partner(me, sign, plane, action):
    z, y, x, c = digits(me)
    base = ((z + 4 + sign * FAR[plane]) % 4) * 32
    inner = [
        ((x + 4 + sign * FAR[i // 2]) % 4) * 2 + (c + 1 - i % 2) % 2 for i in range(8)
    ]

    def row(t, count):
        far = (2 + 3 * ((t * (t + 1)) // 2)) % 4
        start = base + ((y + 4 + sign * far) % 4) * 8
        for i in range(count):
            action(plane * 32 + t * 8 + i, start + inner[i])

    def step(t, carry):
        row(t, 8)
        return carry

    last = plane == PLANES - 1
    lax.fori_loop(0, 3 if last else 4, step, 0)
    if last:
        row(3, 7)


def slot_experts(me, r):
    z, y, x, c = digits(me)
    j = r >> 1

    def far(t):
        return (2 + 3 * ((t * (t + 1)) >> 1)) & 3

    return (
        ((z + far(j >> 5)) & 3) * 32
        + ((y + far((j >> 3) & 3)) & 3) * 8
        + ((x + far((j >> 1) & 3)) & 3) * 2
        + ((c + 1 - (j & 1)) & 1)
    )


def rms_scale(values, gains):
    return values * lax.rsqrt(jnp.mean(values * values, axis=-1, keepdims=True) + epsilon) * gains


def layer_kernel(
    tokens_hbm, places_hbm, norm_gain_hbm, query_hbm, key_hbm, value_hbm, gating_hbm, decay_hbm,
    state_hbm, head_gain_hbm, out_hbm, moe_gain_hbm, route_hbm, group_hbm, inner_hbm, gate_hbm,
    up_hbm, down_hbm, inverse_hbm,
    out_ref, state,
    tokens, places, norm_gain, decay, head_gain, moe_gain, route, group, inner, inverse,
    w_query, w_key, w_value, w_gating, w_out, w_gate, w_up, w_down,
    keys_t, queries_t, values_h, decay_h, reading,
    token_out, token_in, mixed_out, mixed_in, results, returned,
    small_sems, weight_sems, state_sems,
    send_tok, recv_tok, send_mix, recv_mix, send_res, recv_res,
):
    me = lax.axis_index("ep")
    rows, width = tokens.shape
    heads, head_width = values_h.shape[1:]
    n = token_out.shape[0]
    slots = 2 * n
    plane_slots = n // PLANES
    per = n // CHUNKS
    blocks = rows // STATE_BLOCK

    def start(source, target, sem):
        copy = pltpu.make_async_copy(source, target, sem)
        copy.start()
        return copy

    smalls = [
        start(s, t, small_sems.at[i])
        for i, (s, t) in enumerate(
            (
                (group_hbm, group), (inner_hbm, inner), (tokens_hbm, tokens),
                (norm_gain_hbm, norm_gain), (places_hbm, places), (inverse_hbm, inverse),
                (decay_hbm, decay), (head_gain_hbm, head_gain), (moe_gain_hbm, moe_gain),
                (route_hbm, route),
            )
        )
    ]
    weights = [
        start(s, t, weight_sems.at[i])
        for i, (s, t) in enumerate(
            ((key_hbm, w_key), (query_hbm, w_query), (value_hbm, w_value), (gating_hbm, w_gating))
        )
    ]
    barrier = pltpu.get_barrier_semaphore()

    def greet(slot, device):
        pl.semaphore_signal(barrier, inc=1, device_id=(device,), device_id_type=MESH)

    for plane in range(PLANES):
        each_partner(me, 1, plane, greet)
    loads = [
        start(
            state_hbm.at[pl.ds(i * STATE_BLOCK, STATE_BLOCK)],
            state.at[pl.ds(i * STATE_BLOCK, STATE_BLOCK)],
            state_sems.at[i],
        )
        for i in range(blocks)
    ]
    weights += [
        start(s, t, weight_sems.at[4 + i])
        for i, (s, t) in enumerate(
            (
                (out_hbm, w_out), (gate_hbm.at[0], w_gate), (up_hbm.at[0], w_up),
                (down_hbm.at[0], w_down),
            )
        )
    ]
    for copy in smalls:
        copy.wait()

    first_row = group[...] * GROUP_SIZE + inner[0:1, :]
    second_row = group[...] * GROUP_SIZE + inner[1:2, :]
    sub = lax.broadcasted_iota(jnp.int32, (rows, rows), 0)
    lane = lax.broadcasted_iota(jnp.int32, (rows, rows), 1)

    def column(row):
        return jnp.sum(jnp.where(sub == lane, row, jnp.zeros_like(row)), axis=1, keepdims=True)

    first_col, second_col = column(first_row), column(second_row)

    def rank(ids_row):
        same = (first_col == ids_row).astype(F32) + (second_col == ids_row).astype(F32)
        return jnp.sum(jnp.where(sub < lane, same, 0.0), axis=0, keepdims=True)

    first_rank, second_rank = rank(first_row), rank(second_row)
    r_col = lax.broadcasted_iota(jnp.int32, (slots, 1), 0)
    expert_col = slot_experts(me, r_col)
    k_col = (r_col & 1).astype(F32)
    place = ((expert_col == first_row) & (k_col == first_rank)) | (
        (expert_col == second_row) & (k_col == second_rank)
    )
    place = place.astype(F32).astype(BF16)
    token_out[...] = (
        jnp.dot(place, tokens[...], preferred_element_type=F32).astype(BF16).reshape(n, 2, width)
    )
    inputs = tokens[...].astype(F32)
    normed = rms_scale(inputs, norm_gain[...]).astype(BF16)
    angles = column(places[...].astype(F32)) * inverse[...]
    cosine = jnp.concatenate([jnp.cos(angles)] * 4, axis=1)
    sine = jnp.concatenate([jnp.sin(angles)] * 4, axis=1)
    pl.semaphore_wait(barrier, n - 1)

    def remote(source, target, send_sem, recv_sems):
        def action(slot, device):
            pltpu.make_async_remote_copy(
                src_ref=source.at[slot], dst_ref=target.at[slot], send_sem=send_sem,
                recv_sem=recv_sems, device_id=(device,), device_id_type=MESH,
            ).start()

        return action

    for plane in range(PLANES):
        chunk = plane * CHUNKS // PLANES
        each_partner(me, 1, plane, remote(token_out, token_in, send_tok, recv_tok.at[chunk]))
    token_in[n - 1] = token_out[n - 1]

    def project(index, weight):
        weights[index].wait()
        return jnp.dot(normed, weight[...], preferred_element_type=F32).astype(BF16).astype(F32)

    first_half = (lax.broadcasted_iota(jnp.int32, (1, heads * head_width), 1) % head_width) < (
        head_width // 2
    )

    def rotate(x):
        total = heads * head_width
        half = head_width // 2
        swapped = jnp.where(first_half, -pltpu.roll(x, total - half, 1), pltpu.roll(x, half, 1))
        return x * cosine + swapped * sine

    def transposed(x):
        pad = jnp.zeros((128 - rows, x.shape[1]), F32)
        return jnp.concatenate([x, pad], axis=0).T

    keys_t[...] = transposed(rotate(project(0, w_key)) * head_width ** (-0.5))
    queries_t[...] = transposed(rotate(project(1, w_query)))
    values_h[...] = project(2, w_value).reshape(rows, heads, head_width)
    gating = project(3, w_gating)
    retain = jnp.exp(-decay[...])
    decay_h[...] = jnp.concatenate(
        [jnp.broadcast_to(retain[:, h : h + 1], (1, head_width)) for h in range(heads)], axis=0
    )

    def sequence(s, carry):
        index = jnp.full((head_width, 128), s, jnp.int32)
        for h in range(heads):
            part = pl.ds(h * head_width, head_width)

            def spread(ref):
                picked = jnp.take_along_axis(ref[part], index, axis=1, mode="promise_in_bounds")
                return picked[:, :head_width]

            new = decay_h[h : h + 1] * state[s, h] + spread(keys_t) * values_h[s, h : h + 1]
            state[s, h] = new
            reading[s, h : h + 1] = jnp.sum(spread(queries_t) * new, axis=0, keepdims=True)
        return carry

    for i in range(blocks):
        loads[i].wait()
        lax.fori_loop(i * STATE_BLOCK, (i + 1) * STATE_BLOCK, sequence, 0)

    read = reading[...]
    read = read * lax.rsqrt(jnp.mean(read * read, axis=-1, keepdims=True) + epsilon)
    read = read.reshape(rows, heads * head_width) * head_gain[...]
    mixed = (read * (gating * jax.nn.sigmoid(gating))).astype(BF16)
    mixed_out[...] = (
        jnp.dot(place, mixed, preferred_element_type=F32)
        .astype(BF16)
        .reshape(n, 2, mixed.shape[1])
    )
    for plane in range(PLANES):
        chunk = plane * CHUNKS // PLANES
        each_partner(me, 1, plane, remote(mixed_out, mixed_in, send_mix, recv_mix.at[chunk]))
    mixed_in[n - 1] = mixed_out[n - 1]
    weights[4].wait()

    def mix(rows_in, mixed_rows):
        added = jnp.dot(mixed_rows, w_out[...], preferred_element_type=F32)
        return (rows_in.astype(F32) + added).astype(BF16).astype(F32)

    own_tokens = mix(tokens[...], mixed)
    for copy in weights[5:]:
        copy.wait()

    r_row = lax.broadcasted_iota(jnp.int32, (1, slots), 1)
    expert_row = slot_experts(me, r_row)
    k_row = (r_row & 1).astype(F32)
    route_one, route_two = column(route[0:1, :]), column(route[1:2, :])
    first_k, second_k = column(first_rank), column(second_rank)
    scale = jnp.where(
        (first_col == expert_row) & (first_k == k_row), route_one, 0.0
    ) + jnp.where((second_col == expert_row) & (second_k == k_row), route_two, 0.0)
    high = scale.astype(BF16)
    low = (scale - high.astype(F32)).astype(BF16)

    def wait_block(ref, sem, begin, count):
        block = ref.at[pl.ds(begin, count)]
        pltpu.make_async_copy(block, block, sem).wait()

    for chunk in range(CHUNKS):
        begin = chunk * per
        count = per if chunk < CHUNKS - 1 else per - 1
        wait_block(token_in, recv_tok.at[chunk], begin, count)
        wait_block(mixed_in, recv_mix.at[chunk], begin, count)
        x = mix(
            token_in[pl.ds(begin, per)].reshape(2 * per, width),
            mixed_in[pl.ds(begin, per)].reshape(2 * per, mixed.shape[1]),
        )
        x = rms_scale(x, moe_gain[...]).astype(BF16)
        gate_part = jnp.dot(x, w_gate[...], preferred_element_type=F32)
        up_part = jnp.dot(x, w_up[...], preferred_element_type=F32)
        hidden = (gate_part * jax.nn.sigmoid(gate_part) * up_part).astype(BF16)
        y = jnp.dot(hidden, w_down[...], preferred_element_type=F32).astype(BF16)
        results[pl.ds(begin, per)] = y.reshape(per, 2, width)
        for plane in range(chunk * PLANES // CHUNKS, (chunk + 1) * PLANES // CHUNKS):
            each_partner(me, -1, plane, remote(results, returned, send_res, recv_res))
    returned[n - 1] = results[n - 1]

    wait_block(returned, recv_res, 0, n - 1)
    back = returned[...].reshape(slots, width)
    routed = jnp.dot(high, back, preferred_element_type=F32) + jnp.dot(
        low, back, preferred_element_type=F32
    )
    out_ref[...] = (own_tokens + routed).astype(BF16)
    wait_block(token_out, send_tok, 0, n - 1)
    wait_block(mixed_out, send_mix, 0, n - 1)
    wait_block(results, send_res, 0, n - 1)


def local(
    tokens, history_length, norm_gain, w_query, w_key, w_value, w_gate, decay_rate, state,
    head_gain, w_out, moe_gain, route_weights, expert_group, expert_inner, expert_gate,
    expert_up, expert_down,
):
    n = lax.axis_size("ep")
    rows, width = tokens.shape
    heads, head_width = state.shape[1], state.shape[2]
    ret_width = w_query.shape[1]
    hidden = expert_gate.shape[2]
    half = head_width // 2
    inverse = 10000.0 ** (-(np.arange(128) % half).astype(np.float64) / half)
    inverse = jnp.asarray(inverse.astype(np.float32)[None])
    operands = (
        tokens, history_length.reshape(1, rows), norm_gain.reshape(1, width), w_query, w_key,
        w_value, w_gate, decay_rate.reshape(1, heads), state, head_gain.reshape(1, ret_width),
        w_out, moe_gain.reshape(1, width), route_weights.T, expert_group.reshape(1, rows),
        expert_inner.T, expert_gate, expert_up, expert_down, inverse,
    )
    vmem = pl.BlockSpec(memory_space=pltpu.VMEM)
    hbm = pl.BlockSpec(memory_space=pltpu.HBM)
    V = pltpu.VMEM
    DMA = pltpu.SemaphoreType.DMA
    output, new_state = pl.pallas_call(
        layer_kernel,
        out_shape=(jax.ShapeDtypeStruct((rows, width), BF16), V(state.shape, F32)),
        in_specs=[hbm] * len(operands),
        out_specs=(vmem, vmem),
        scratch_shapes=[
            V((rows, width), BF16), V((1, rows), jnp.int32), V((1, width), F32),
            V((1, heads), F32), V((1, ret_width), F32), V((1, width), F32),
            V((2, rows), F32), V((1, rows), jnp.int32), V((2, rows), jnp.int32), V((1, 128), F32),
            V((width, ret_width), BF16), V((width, ret_width), BF16),
            V((width, ret_width), BF16), V((width, ret_width), BF16),
            V((ret_width, width), BF16), V((width, hidden), BF16), V((width, hidden), BF16),
            V((hidden, width), BF16),
            V((ret_width, 128), F32), V((ret_width, 128), F32), V((rows, heads, head_width), F32),
            V((heads, head_width), F32), V((rows, heads, head_width), F32),
            V((n, 2, width), BF16), V((n, 2, width), BF16),
            V((n, 2, ret_width), BF16), V((n, 2, ret_width), BF16),
            V((n, 2, width), BF16), V((n, 2, width), BF16),
            DMA((10,)), DMA((8,)), DMA((rows // STATE_BLOCK,)),
            DMA, DMA((CHUNKS,)), DMA, DMA((CHUNKS,)), DMA, DMA,
        ],
        compiler_params=pltpu.CompilerParams(
            collective_id=0, has_side_effects=True, vmem_limit_bytes=46 * 1024 * 1024
        ),
    )(*operands)
    return (output, new_state)


def solution(mesh):
    return jax.shard_map(
        local,
        mesh=mesh,
        in_specs=(
            P("ep", None), P("ep"), P(), P(), P(), P(), P(), P(), P("ep", None, None, None),
            P(), P(), P(), P("ep", None), P("ep"), P("ep", None), P("ep", None, None),
            P("ep", None, None), P("ep", None, None),
        ),
        out_specs=(P("ep", None), P("ep", None, None, None)),
        check_vma=False,
    )
```

```python
import numpy as np

import jax
import jax.numpy as jnp
from jax import lax
from jax.experimental import pallas as pl
from jax.experimental.pallas import tpu as pltpu
from jax.sharding import PartitionSpec as P

MESH = pl.DeviceIdType.MESH
F32 = jnp.float32
BF16 = jnp.bfloat16
GROUP_SIZE = 32
PLANES = 4
CHUNKS = 4
STATE_BLOCK = 8
epsilon = 1e-06


FAR = (2, 1, 3, 0)


def digits(me):
    return me // 32, (me // 8) % 4, (me // 2) % 4, me % 2


def each_partner(me, sign, plane, action):
    z, y, x, c = digits(me)
    base = ((z + 4 + sign * FAR[plane]) % 4) * 32
    inner = [
        ((x + 4 + sign * FAR[i // 2]) % 4) * 2 + (c + 1 - i % 2) % 2 for i in range(8)
    ]

    def row(t, count):
        far = (2 + 3 * ((t * (t + 1)) // 2)) % 4
        start = base + ((y + 4 + sign * far) % 4) * 8
        for i in range(count):
            action(plane * 32 + t * 8 + i, start + inner[i])

    def step(t, carry):
        row(t, 8)
        return carry

    last = plane == PLANES - 1
    lax.fori_loop(0, 3 if last else 4, step, 0)
    if last:
        row(3, 7)


def slot_experts(me, r):
    z, y, x, c = digits(me)
    j = r >> 1

    def far(t):
        return (2 + 3 * ((t * (t + 1)) >> 1)) & 3

    return (
        ((z + far(j >> 5)) & 3) * 32
        + ((y + far((j >> 3) & 3)) & 3) * 8
        + ((x + far((j >> 1) & 3)) & 3) * 2
        + ((c + 1 - (j & 1)) & 1)
    )


def rms_scale(values, gains):
    return values * lax.rsqrt(jnp.mean(values * values, axis=-1, keepdims=True) + epsilon) * gains


def layer_kernel(
    tokens_hbm, places_hbm, norm_gain_hbm, query_hbm, key_hbm, value_hbm, gating_hbm, decay_hbm,
    state_hbm, head_gain_hbm, out_hbm, moe_gain_hbm, route_hbm, group_hbm, inner_hbm, gate_hbm,
    up_hbm, down_hbm, inverse_hbm,
    out_ref, state,
    tokens, places, norm_gain, decay, head_gain, moe_gain, route, group, inner, inverse,
    w_query, w_key, w_value, w_gating, w_out, w_gate, w_up, w_down,
    keys_t, queries, values_h, decay_h, reading,
    token_out, token_in, mixed_out, mixed_in, results, returned,
    small_sems, weight_sems, state_sems,
    send_tok, recv_tok, send_mix, recv_mix, send_res, recv_res,
):
    me = lax.axis_index("ep")
    rows, width = tokens.shape
    heads, head_width = values_h.shape[1:]
    n = token_out.shape[0]
    slots = 2 * n
    plane_slots = n // PLANES
    per = n // CHUNKS
    blocks = rows // STATE_BLOCK

    def start(source, target, sem):
        copy = pltpu.make_async_copy(source, target, sem)
        copy.start()
        return copy

    smalls = [
        start(s, t, small_sems.at[i])
        for i, (s, t) in enumerate(
            (
                (group_hbm, group), (inner_hbm, inner), (tokens_hbm, tokens),
                (norm_gain_hbm, norm_gain), (places_hbm, places), (inverse_hbm, inverse),
                (decay_hbm, decay), (head_gain_hbm, head_gain), (moe_gain_hbm, moe_gain),
                (route_hbm, route),
            )
        )
    ]
    weights = [
        start(s, t, weight_sems.at[i])
        for i, (s, t) in enumerate(
            ((key_hbm, w_key), (query_hbm, w_query), (value_hbm, w_value), (gating_hbm, w_gating))
        )
    ]
    barrier = pltpu.get_barrier_semaphore()

    def greet(slot, device):
        pl.semaphore_signal(barrier, inc=1, device_id=(device,), device_id_type=MESH)

    for plane in range(PLANES):
        each_partner(me, 1, plane, greet)
    loads = [
        start(
            state_hbm.at[pl.ds(i * STATE_BLOCK, STATE_BLOCK)],
            state.at[pl.ds(i * STATE_BLOCK, STATE_BLOCK)],
            state_sems.at[i],
        )
        for i in range(blocks)
    ]
    weights += [
        start(s, t, weight_sems.at[4 + i])
        for i, (s, t) in enumerate(
            (
                (out_hbm, w_out), (gate_hbm.at[0], w_gate), (up_hbm.at[0], w_up),
                (down_hbm.at[0], w_down),
            )
        )
    ]
    for copy in smalls:
        copy.wait()

    first_row = group[...] * GROUP_SIZE + inner[0:1, :]
    second_row = group[...] * GROUP_SIZE + inner[1:2, :]
    sub = lax.broadcasted_iota(jnp.int32, (rows, rows), 0)
    lane = lax.broadcasted_iota(jnp.int32, (rows, rows), 1)

    def column(row):
        return jnp.sum(jnp.where(sub == lane, row, jnp.zeros_like(row)), axis=1, keepdims=True)

    first_col, second_col = column(first_row), column(second_row)

    def rank(ids_row):
        same = (first_col == ids_row).astype(F32) + (second_col == ids_row).astype(F32)
        return jnp.sum(jnp.where(sub < lane, same, 0.0), axis=0, keepdims=True)

    first_rank, second_rank = rank(first_row), rank(second_row)
    r_col = lax.broadcasted_iota(jnp.int32, (slots, 1), 0)
    expert_col = slot_experts(me, r_col)
    k_col = (r_col & 1).astype(F32)
    place = ((expert_col == first_row) & (k_col == first_rank)) | (
        (expert_col == second_row) & (k_col == second_rank)
    )
    place = place.astype(F32).astype(BF16)
    token_out[...] = (
        jnp.dot(place, tokens[...], preferred_element_type=F32).astype(BF16).reshape(n, 2, width)
    )
    inputs = tokens[...].astype(F32)
    normed = rms_scale(inputs, norm_gain[...]).astype(BF16)
    angles = column(places[...].astype(F32)) * inverse[...]
    cosine = jnp.concatenate([jnp.cos(angles)] * 4, axis=1)
    sine = jnp.concatenate([jnp.sin(angles)] * 4, axis=1)
    pl.semaphore_wait(barrier, n - 1)

    def remote(source, target, send_sem, recv_sems):
        def action(slot, device):
            pltpu.make_async_remote_copy(
                src_ref=source.at[slot], dst_ref=target.at[slot], send_sem=send_sem,
                recv_sem=recv_sems, device_id=(device,), device_id_type=MESH,
            ).start()

        return action

    for plane in range(PLANES):
        chunk = plane * CHUNKS // PLANES
        each_partner(me, 1, plane, remote(token_out, token_in, send_tok, recv_tok.at[chunk]))
    token_in[n - 1] = token_out[n - 1]

    def project(index, weight):
        weights[index].wait()
        return jnp.dot(normed, weight[...], preferred_element_type=F32).astype(BF16).astype(F32)

    first_half = (lax.broadcasted_iota(jnp.int32, (1, heads * head_width), 1) % head_width) < (
        head_width // 2
    )

    def rotate(x):
        total = heads * head_width
        half = head_width // 2
        swapped = jnp.where(first_half, -pltpu.roll(x, total - half, 1), pltpu.roll(x, half, 1))
        return x * cosine + swapped * sine

    def transposed(x):
        pad = jnp.zeros((128 - rows, x.shape[1]), F32)
        return jnp.concatenate([x, pad], axis=0).T

    keys_t[...] = transposed(rotate(project(0, w_key)) * head_width ** (-0.5))
    query = rotate(project(1, w_query))
    query_high = query.astype(BF16).astype(F32)
    head_of = lax.broadcasted_iota(jnp.int32, (1, heads, heads * head_width), 2) // head_width
    head_row = lax.broadcasted_iota(jnp.int32, (1, heads, heads * head_width), 1)
    for i, piece in enumerate((query_high, query - query_high)):
        queries[:, pl.ds(i * heads, heads)] = jnp.where(
            head_of == head_row, piece[:, None, :], 0.0
        ).astype(BF16)
    values_h[...] = project(2, w_value).reshape(rows, heads, head_width)
    gating = project(3, w_gating)
    retain = jnp.exp(-decay[...])
    decay_h[...] = jnp.concatenate(
        [jnp.broadcast_to(retain[:, h : h + 1], (1, head_width)) for h in range(heads)], axis=0
    )

    def sequence(s, carry):
        index = jnp.full((head_width, 128), s, jnp.int32)
        rounded = []
        for h in range(heads):
            key = jnp.take_along_axis(
                keys_t[pl.ds(h * head_width, head_width)], index, axis=1, mode="promise_in_bounds"
            )[:, :head_width]
            new = decay_h[h : h + 1] * state[s, h] + key * values_h[s, h : h + 1]
            state[s, h] = new
            rounded.append(new.astype(BF16))
        read = jnp.dot(
            queries[s], jnp.concatenate(rounded, axis=0), preferred_element_type=F32
        )
        reading[s] = read[:heads] + read[heads:]
        return carry

    for i in range(blocks):
        loads[i].wait()
        lax.fori_loop(
            i * STATE_BLOCK, (i + 1) * STATE_BLOCK, sequence, 0, unroll=STATE_BLOCK
        )

    read = reading[...]
    read = read * lax.rsqrt(jnp.mean(read * read, axis=-1, keepdims=True) + epsilon)
    read = read.reshape(rows, heads * head_width) * head_gain[...]
    mixed = (read * (gating * jax.nn.sigmoid(gating))).astype(BF16)
    mixed_out[...] = (
        jnp.dot(place, mixed, preferred_element_type=F32)
        .astype(BF16)
        .reshape(n, 2, mixed.shape[1])
    )
    for plane in range(PLANES):
        chunk = plane * CHUNKS // PLANES
        each_partner(me, 1, plane, remote(mixed_out, mixed_in, send_mix, recv_mix.at[chunk]))
    mixed_in[n - 1] = mixed_out[n - 1]
    weights[4].wait()

    def mix(rows_in, mixed_rows):
        added = jnp.dot(mixed_rows, w_out[...], preferred_element_type=F32)
        return (rows_in.astype(F32) + added).astype(BF16).astype(F32)

    own_tokens = mix(tokens[...], mixed)
    for copy in weights[5:]:
        copy.wait()

    r_row = lax.broadcasted_iota(jnp.int32, (1, slots), 1)
    expert_row = slot_experts(me, r_row)
    k_row = (r_row & 1).astype(F32)
    route_one, route_two = column(route[0:1, :]), column(route[1:2, :])
    first_k, second_k = column(first_rank), column(second_rank)
    scale = jnp.where(
        (first_col == expert_row) & (first_k == k_row), route_one, 0.0
    ) + jnp.where((second_col == expert_row) & (second_k == k_row), route_two, 0.0)
    high = scale.astype(BF16)
    low = (scale - high.astype(F32)).astype(BF16)

    def wait_block(ref, sem, begin, count):
        block = ref.at[pl.ds(begin, count)]
        pltpu.make_async_copy(block, block, sem).wait()

    for chunk in range(CHUNKS):
        begin = chunk * per
        count = per if chunk < CHUNKS - 1 else per - 1
        wait_block(token_in, recv_tok.at[chunk], begin, count)
        wait_block(mixed_in, recv_mix.at[chunk], begin, count)
        x = mix(
            token_in[pl.ds(begin, per)].reshape(2 * per, width),
            mixed_in[pl.ds(begin, per)].reshape(2 * per, mixed.shape[1]),
        )
        x = rms_scale(x, moe_gain[...]).astype(BF16)
        gate_part = jnp.dot(x, w_gate[...], preferred_element_type=F32)
        up_part = jnp.dot(x, w_up[...], preferred_element_type=F32)
        hidden = (gate_part * jax.nn.sigmoid(gate_part) * up_part).astype(BF16)
        y = jnp.dot(hidden, w_down[...], preferred_element_type=F32).astype(BF16)
        results[pl.ds(begin, per)] = y.reshape(per, 2, width)
        for plane in range(chunk * PLANES // CHUNKS, (chunk + 1) * PLANES // CHUNKS):
            each_partner(me, -1, plane, remote(results, returned, send_res, recv_res))
    returned[n - 1] = results[n - 1]

    wait_block(returned, recv_res, 0, n - 1)
    back = returned[...].reshape(slots, width)
    routed = jnp.dot(high, back, preferred_element_type=F32) + jnp.dot(
        low, back, preferred_element_type=F32
    )
    out_ref[...] = (own_tokens + routed).astype(BF16)
    wait_block(token_out, send_tok, 0, n - 1)
    wait_block(mixed_out, send_mix, 0, n - 1)
    wait_block(results, send_res, 0, n - 1)


def write_kernel(output, new_state, output_hbm, state_hbm, sems):
    pieces = sems.shape[0] - 1
    size = new_state.shape[0] // pieces
    copies = [
        pltpu.make_async_copy(
            new_state.at[pl.ds(i * size, size)], state_hbm.at[pl.ds(i * size, size)], sems.at[i]
        )
        for i in range(pieces)
    ]
    copies.append(pltpu.make_async_copy(output, output_hbm, sems.at[pieces]))
    for copy in copies:
        copy.start()
    for copy in copies:
        copy.wait()


def local(
    tokens, history_length, norm_gain, w_query, w_key, w_value, w_gate, decay_rate, state,
    head_gain, w_out, moe_gain, route_weights, expert_group, expert_inner, expert_gate,
    expert_up, expert_down,
):
    n = lax.axis_size("ep")
    rows, width = tokens.shape
    heads, head_width = state.shape[1], state.shape[2]
    ret_width = w_query.shape[1]
    hidden = expert_gate.shape[2]
    half = head_width // 2
    inverse = 10000.0 ** (-(np.arange(128) % half).astype(np.float64) / half)
    inverse = jnp.asarray(inverse.astype(np.float32)[None])
    operands = (
        tokens, history_length.reshape(1, rows), norm_gain.reshape(1, width), w_query, w_key,
        w_value, w_gate, decay_rate.reshape(1, heads), state, head_gain.reshape(1, ret_width),
        w_out, moe_gain.reshape(1, width), route_weights.T, expert_group.reshape(1, rows),
        expert_inner.T, expert_gate, expert_up, expert_down, inverse,
    )
    vmem = pl.BlockSpec(memory_space=pltpu.VMEM)
    hbm = pl.BlockSpec(memory_space=pltpu.HBM)
    V = pltpu.VMEM
    DMA = pltpu.SemaphoreType.DMA
    output, new_state = pl.pallas_call(
        layer_kernel,
        out_shape=(V((rows, width), BF16), V(state.shape, F32)),
        in_specs=[hbm] * len(operands),
        out_specs=(vmem, vmem),
        scratch_shapes=[
            V((rows, width), BF16), V((1, rows), jnp.int32), V((1, width), F32),
            V((1, heads), F32), V((1, ret_width), F32), V((1, width), F32),
            V((2, rows), F32), V((1, rows), jnp.int32), V((2, rows), jnp.int32), V((1, 128), F32),
            V((width, ret_width), BF16), V((width, ret_width), BF16),
            V((width, ret_width), BF16), V((width, ret_width), BF16),
            V((ret_width, width), BF16), V((width, hidden), BF16), V((width, hidden), BF16),
            V((hidden, width), BF16),
            V((ret_width, 128), F32), V((rows, 2 * heads, ret_width), BF16),
            V((rows, heads, head_width), F32),
            V((heads, head_width), F32), V((rows, heads, head_width), F32),
            V((n, 2, width), BF16), V((n, 2, width), BF16),
            V((n, 2, ret_width), BF16), V((n, 2, ret_width), BF16),
            V((n, 2, width), BF16), V((n, 2, width), BF16),
            DMA((10,)), DMA((8,)), DMA((rows // STATE_BLOCK,)),
            DMA, DMA((CHUNKS,)), DMA, DMA((CHUNKS,)), DMA, DMA,
        ],
        compiler_params=pltpu.CompilerParams(
            collective_id=0, has_side_effects=True, vmem_limit_bytes=46 * 1024 * 1024
        ),
    )(*operands)
    pieces = 8
    return pl.pallas_call(
        write_kernel,
        out_shape=(
            jax.ShapeDtypeStruct((rows, width), BF16), jax.ShapeDtypeStruct(state.shape, F32),
        ),
        in_specs=[vmem, vmem],
        out_specs=(hbm, hbm),
        scratch_shapes=[DMA((pieces + 1,))],
        compiler_params=pltpu.CompilerParams(vmem_limit_bytes=1024 * 1024),
    )(
        pltpu.with_memory_space_constraint(output, pltpu.VMEM),
        pltpu.with_memory_space_constraint(new_state, pltpu.VMEM),
    )


def solution(mesh):
    return jax.shard_map(
        local,
        mesh=mesh,
        in_specs=(
            P("ep", None), P("ep"), P(), P(), P(), P(), P(), P(), P("ep", None, None, None),
            P(), P(), P(), P("ep", None), P("ep"), P("ep", None), P("ep", None, None),
            P("ep", None, None), P("ep", None, None),
        ),
        out_specs=(P("ep", None), P("ep", None, None, None)),
        check_vma=False,
    )
```

```python
import numpy as np

import jax
import jax.numpy as jnp
from jax import lax
from jax.experimental import pallas as pl
from jax.experimental.pallas import tpu as pltpu
from jax.sharding import PartitionSpec as P

MESH = pl.DeviceIdType.MESH
F32 = jnp.float32
BF16 = jnp.bfloat16
GROUP_SIZE = 32
PLANES = 4
EARLY = 2
STATE_BLOCK = 8
epsilon = 1e-06


FAR = (2, 1, 3, 0)


def digits(me):
    return me // 32, (me // 8) % 4, (me // 2) % 4, me % 2


def each_partner(me, sign, plane, action):
    z, y, x, c = digits(me)
    planes = [((z + 4 + sign * far) % 4) * 32 for far in FAR]
    lines = [((y + 4 + sign * far) % 4) * 8 for far in FAR]
    inner = [
        ((x + 4 + sign * FAR[i // 2]) % 4) * 2 + (c + 1 - i % 2) % 2 for i in range(8)
    ]
    for i in range(31 if plane == PLANES - 1 else 32):
        t = i // 8
        offset = (plane + 2 - t - (i % 8) // 2) % 4
        action(plane * 32 + i, planes[offset] + lines[t] + inner[i % 8])


def slot_experts(me, r):
    z, y, x, c = digits(me)
    j = r >> 1

    def far(t):
        return (2 + 3 * ((t * (t + 1)) >> 1)) & 3

    return (
        ((z + far(((j >> 5) + 2 - (j >> 3) - (j >> 1)) & 3)) & 3) * 32
        + ((y + far((j >> 3) & 3)) & 3) * 8
        + ((x + far((j >> 1) & 3)) & 3) * 2
        + ((c + 1 - (j & 1)) & 1)
    )


def rms_scale(values, gains):
    return values * lax.rsqrt(jnp.mean(values * values, axis=-1, keepdims=True) + epsilon) * gains


def layer_kernel(
    tokens_hbm, places_hbm, norm_gain_hbm, query_hbm, key_hbm, value_hbm, gating_hbm, decay_hbm,
    state_hbm, head_gain_hbm, out_hbm, moe_gain_hbm, route_hbm, group_hbm, inner_hbm, gate_hbm,
    up_hbm, down_hbm, inverse_hbm,
    out_ref, state,
    tokens, places, norm_gain, decay, head_gain, moe_gain, route, group, inner, inverse,
    w_query, w_key, w_value, w_gating, w_out, w_gate, w_up, w_down,
    keys_t, queries, values_h, decay_h, reading,
    token_out, token_in, mixed_out, mixed_in, results, returned,
    small_sems, weight_sems, state_sems,
    send_tok, recv_tok, send_mix, recv_mix, send_res, recv_res,
):
    me = lax.axis_index("ep")
    rows, width = tokens.shape
    heads, head_width = values_h.shape[1:]
    n = token_out.shape[0]
    slots = 2 * n
    per = n // PLANES
    early = EARLY * per
    blocks = rows // STATE_BLOCK

    def start(source, target, sem):
        copy = pltpu.make_async_copy(source, target, sem)
        copy.start()
        return copy

    smalls = [
        start(s, t, small_sems.at[i])
        for i, (s, t) in enumerate(
            (
                (group_hbm, group), (inner_hbm, inner), (tokens_hbm, tokens),
                (norm_gain_hbm, norm_gain), (places_hbm, places), (inverse_hbm, inverse),
                (decay_hbm, decay), (head_gain_hbm, head_gain), (moe_gain_hbm, moe_gain),
                (route_hbm, route),
            )
        )
    ]
    weights = [
        start(s, t, weight_sems.at[i])
        for i, (s, t) in enumerate(
            ((key_hbm, w_key), (query_hbm, w_query), (value_hbm, w_value), (gating_hbm, w_gating))
        )
    ]
    barrier = pltpu.get_barrier_semaphore()

    def greet(slot, device):
        pl.semaphore_signal(barrier, inc=1, device_id=(device,), device_id_type=MESH)

    for plane in range(PLANES):
        each_partner(me, 1, plane, greet)
    loads = [
        start(
            state_hbm.at[pl.ds(i * STATE_BLOCK, STATE_BLOCK)],
            state.at[pl.ds(i * STATE_BLOCK, STATE_BLOCK)],
            state_sems.at[i],
        )
        for i in range(blocks)
    ]
    weights += [
        start(s, t, weight_sems.at[4 + i])
        for i, (s, t) in enumerate(
            (
                (out_hbm, w_out), (gate_hbm.at[0], w_gate), (up_hbm.at[0], w_up),
                (down_hbm.at[0], w_down),
            )
        )
    ]
    for copy in smalls:
        copy.wait()

    first_row = group[...] * GROUP_SIZE + inner[0:1, :]
    second_row = group[...] * GROUP_SIZE + inner[1:2, :]
    sub = lax.broadcasted_iota(jnp.int32, (rows, rows), 0)
    lane = lax.broadcasted_iota(jnp.int32, (rows, rows), 1)

    def column(row):
        return jnp.sum(jnp.where(sub == lane, row, jnp.zeros_like(row)), axis=1, keepdims=True)

    first_col, second_col = column(first_row), column(second_row)

    def rank(ids_row):
        same = (first_col == ids_row).astype(F32) + (second_col == ids_row).astype(F32)
        return jnp.sum(jnp.where(sub < lane, same, 0.0), axis=0, keepdims=True)

    first_rank, second_rank = rank(first_row), rank(second_row)
    r_col = lax.broadcasted_iota(jnp.int32, (slots, 1), 0)
    expert_col = slot_experts(me, r_col)
    k_col = (r_col & 1).astype(F32)
    place = ((expert_col == first_row) & (k_col == first_rank)) | (
        (expert_col == second_row) & (k_col == second_rank)
    )
    place = place.astype(F32).astype(BF16)

    def slab(chosen, values):
        taken = jnp.dot(chosen, values, preferred_element_type=F32).astype(BF16)
        return taken.reshape(chosen.shape[0] // 2, 2, values.shape[1])

    token_out[pl.ds(0, early)] = slab(place[: 2 * early], tokens[...])
    inputs = tokens[...].astype(F32)
    normed = rms_scale(inputs, norm_gain[...]).astype(BF16)
    angles = column(places[...].astype(F32)) * inverse[...]
    cosine = jnp.concatenate([jnp.cos(angles)] * 4, axis=1)
    sine = jnp.concatenate([jnp.sin(angles)] * 4, axis=1)

    def remote(source, target, send_sem, recv_sems):
        def action(slot, device):
            pltpu.make_async_remote_copy(
                src_ref=source.at[slot], dst_ref=target.at[slot], send_sem=send_sem,
                recv_sem=recv_sems, device_id=(device,), device_id_type=MESH,
            ).start()

        return action


    def project(index, weight):
        weights[index].wait()
        return jnp.dot(normed, weight[...], preferred_element_type=F32).astype(BF16).astype(F32)

    first_half = (lax.broadcasted_iota(jnp.int32, (1, heads * head_width), 1) % head_width) < (
        head_width // 2
    )

    def rotate(x):
        total = heads * head_width
        half = head_width // 2
        swapped = jnp.where(first_half, -pltpu.roll(x, total - half, 1), pltpu.roll(x, half, 1))
        return x * cosine + swapped * sine

    def transposed(x):
        pad = jnp.zeros((128 - rows, x.shape[1]), F32)
        return jnp.concatenate([x, pad], axis=0).T

    keys_t[...] = transposed(rotate(project(0, w_key)) * head_width ** (-0.5))
    query = rotate(project(1, w_query))
    query_high = query.astype(BF16).astype(F32)
    head_of = lax.broadcasted_iota(jnp.int32, (1, heads, heads * head_width), 2) // head_width
    head_row = lax.broadcasted_iota(jnp.int32, (1, heads, heads * head_width), 1)
    for i, piece in enumerate((query_high, query - query_high)):
        queries[:, pl.ds(i * heads, heads)] = jnp.where(
            head_of == head_row, piece[:, None, :], 0.0
        ).astype(BF16)
    values_h[...] = project(2, w_value).reshape(rows, heads, head_width)
    gating = project(3, w_gating)
    retain = jnp.exp(-decay[...])
    decay_h[...] = jnp.concatenate(
        [jnp.broadcast_to(retain[:, h : h + 1], (1, head_width)) for h in range(heads)], axis=0
    )

    def sequence(s, carry):
        index = jnp.full((head_width, 128), s, jnp.int32)
        rounded = []
        for h in range(heads):
            key = jnp.take_along_axis(
                keys_t[pl.ds(h * head_width, head_width)], index, axis=1, mode="promise_in_bounds"
            )[:, :head_width]
            new = decay_h[h : h + 1] * state[s, h] + key * values_h[s, h : h + 1]
            state[s, h] = new
            rounded.append(new.astype(BF16))
        read = jnp.dot(
            queries[s], jnp.concatenate(rounded, axis=0), preferred_element_type=F32
        )
        reading[s] = read[:heads] + read[heads:]
        return carry

    pl.semaphore_wait(barrier, n - 1)
    for plane in range(EARLY):
        each_partner(me, 1, plane, remote(token_out, token_in, send_tok, recv_tok.at[plane]))

    for i in range(blocks):
        loads[i].wait()
        lax.fori_loop(
            i * STATE_BLOCK, (i + 1) * STATE_BLOCK, sequence, 0, unroll=STATE_BLOCK
        )

    read = reading[...]
    read = read * lax.rsqrt(jnp.mean(read * read, axis=-1, keepdims=True) + epsilon)
    read = read.reshape(rows, heads * head_width) * head_gain[...]
    mixed = (read * (gating * jax.nn.sigmoid(gating))).astype(BF16)
    mixed_out[pl.ds(0, early)] = slab(place[: 2 * early], mixed)
    for plane in range(EARLY):
        each_partner(me, 1, plane, remote(mixed_out, mixed_in, send_mix, recv_mix.at[plane]))
    weights[4].wait()

    def mix(rows_in, mixed_rows):
        added = jnp.dot(mixed_rows, w_out[...], preferred_element_type=F32)
        return (rows_in.astype(F32) + added).astype(BF16).astype(F32)

    own_tokens = mix(tokens[...], mixed)
    direct = rms_scale(own_tokens, moe_gain[...]).astype(BF16)
    token_out[pl.ds(early, n - early)] = slab(place[2 * early :], direct)
    for plane in range(EARLY, PLANES):
        each_partner(me, 1, plane, remote(token_out, token_in, send_tok, recv_tok.at[plane]))
    token_in[n - 1] = token_out[n - 1]
    for copy in weights[5:]:
        copy.wait()

    r_row = lax.broadcasted_iota(jnp.int32, (1, slots), 1)
    expert_row = slot_experts(me, r_row)
    k_row = (r_row & 1).astype(F32)
    route_one, route_two = column(route[0:1, :]), column(route[1:2, :])
    first_k, second_k = column(first_rank), column(second_rank)
    scale = jnp.where(
        (first_col == expert_row) & (first_k == k_row), route_one, 0.0
    ) + jnp.where((second_col == expert_row) & (second_k == k_row), route_two, 0.0)
    high = scale.astype(BF16)
    low = (scale - high.astype(F32)).astype(BF16)

    def wait_block(ref, sem, begin, count):
        block = ref.at[pl.ds(begin, count)]
        pltpu.make_async_copy(block, block, sem).wait()

    for plane in range(PLANES):
        begin = plane * per
        count = per if plane < PLANES - 1 else per - 1
        wait_block(token_in, recv_tok.at[plane], begin, count)
        x = token_in[pl.ds(begin, per)].reshape(2 * per, width)
        if plane < EARLY:
            wait_block(mixed_in, recv_mix.at[plane], begin, count)
            x = mix(x, mixed_in[pl.ds(begin, per)].reshape(2 * per, mixed.shape[1]))
            x = rms_scale(x, moe_gain[...]).astype(BF16)
        gate_part = jnp.dot(x, w_gate[...], preferred_element_type=F32)
        up_part = jnp.dot(x, w_up[...], preferred_element_type=F32)
        hidden = (gate_part * jax.nn.sigmoid(gate_part) * up_part).astype(BF16)
        y = jnp.dot(hidden, w_down[...], preferred_element_type=F32).astype(BF16)
        results[pl.ds(begin, per)] = y.reshape(per, 2, width)
        each_partner(me, -1, plane, remote(results, returned, send_res, recv_res))
    returned[n - 1] = results[n - 1]

    wait_block(returned, recv_res, 0, n - 1)
    back = returned[...].reshape(slots, width)
    routed = jnp.dot(high, back, preferred_element_type=F32) + jnp.dot(
        low, back, preferred_element_type=F32
    )
    out_ref[...] = (own_tokens + routed).astype(BF16)
    wait_block(token_out, send_tok, 0, n - 1)
    wait_block(mixed_out, send_mix, 0, early)
    wait_block(results, send_res, 0, n - 1)


def write_kernel(output, new_state, output_hbm, state_hbm, sems):
    pieces = sems.shape[0] - 1
    size = new_state.shape[0] // pieces
    copies = [
        pltpu.make_async_copy(
            new_state.at[pl.ds(i * size, size)], state_hbm.at[pl.ds(i * size, size)], sems.at[i]
        )
        for i in range(pieces)
    ]
    copies.append(pltpu.make_async_copy(output, output_hbm, sems.at[pieces]))
    for copy in copies:
        copy.start()
    for copy in copies:
        copy.wait()


def local(
    tokens, history_length, norm_gain, w_query, w_key, w_value, w_gate, decay_rate, state,
    head_gain, w_out, moe_gain, route_weights, expert_group, expert_inner, expert_gate,
    expert_up, expert_down,
):
    n = lax.axis_size("ep")
    rows, width = tokens.shape
    heads, head_width = state.shape[1], state.shape[2]
    ret_width = w_query.shape[1]
    hidden = expert_gate.shape[2]
    half = head_width // 2
    inverse = 10000.0 ** (-(np.arange(128) % half).astype(np.float64) / half)
    inverse = jnp.asarray(inverse.astype(np.float32)[None])
    operands = (
        tokens, history_length.reshape(1, rows), norm_gain.reshape(1, width), w_query, w_key,
        w_value, w_gate, decay_rate.reshape(1, heads), state, head_gain.reshape(1, ret_width),
        w_out, moe_gain.reshape(1, width), route_weights.T, expert_group.reshape(1, rows),
        expert_inner.T, expert_gate, expert_up, expert_down, inverse,
    )
    vmem = pl.BlockSpec(memory_space=pltpu.VMEM)
    hbm = pl.BlockSpec(memory_space=pltpu.HBM)
    V = pltpu.VMEM
    DMA = pltpu.SemaphoreType.DMA
    output, new_state = pl.pallas_call(
        layer_kernel,
        out_shape=(V((rows, width), BF16), V(state.shape, F32)),
        in_specs=[hbm] * len(operands),
        out_specs=(vmem, vmem),
        scratch_shapes=[
            V((rows, width), BF16), V((1, rows), jnp.int32), V((1, width), F32),
            V((1, heads), F32), V((1, ret_width), F32), V((1, width), F32),
            V((2, rows), F32), V((1, rows), jnp.int32), V((2, rows), jnp.int32), V((1, 128), F32),
            V((width, ret_width), BF16), V((width, ret_width), BF16),
            V((width, ret_width), BF16), V((width, ret_width), BF16),
            V((ret_width, width), BF16), V((width, hidden), BF16), V((width, hidden), BF16),
            V((hidden, width), BF16),
            V((ret_width, 128), F32), V((rows, 2 * heads, ret_width), BF16),
            V((rows, heads, head_width), F32),
            V((heads, head_width), F32), V((rows, heads, head_width), F32),
            V((n, 2, width), BF16), V((n, 2, width), BF16),
            V((n, 2, ret_width), BF16), V((n, 2, ret_width), BF16),
            V((n, 2, width), BF16), V((n, 2, width), BF16),
            DMA((10,)), DMA((8,)), DMA((rows // STATE_BLOCK,)),
            DMA, DMA((PLANES,)), DMA, DMA((EARLY,)), DMA, DMA,
        ],
        compiler_params=pltpu.CompilerParams(
            collective_id=0, has_side_effects=True, vmem_limit_bytes=46 * 1024 * 1024
        ),
    )(*operands)
    pieces = 8
    return pl.pallas_call(
        write_kernel,
        out_shape=(
            jax.ShapeDtypeStruct((rows, width), BF16), jax.ShapeDtypeStruct(state.shape, F32),
        ),
        in_specs=[vmem, vmem],
        out_specs=(hbm, hbm),
        scratch_shapes=[DMA((pieces + 1,))],
        compiler_params=pltpu.CompilerParams(vmem_limit_bytes=1024 * 1024),
    )(
        pltpu.with_memory_space_constraint(output, pltpu.VMEM),
        pltpu.with_memory_space_constraint(new_state, pltpu.VMEM),
    )


def solution(mesh):
    return jax.shard_map(
        local,
        mesh=mesh,
        in_specs=(
            P("ep", None), P("ep"), P(), P(), P(), P(), P(), P(), P("ep", None, None, None),
            P(), P(), P(), P("ep", None), P("ep"), P("ep", None), P("ep", None, None),
            P("ep", None, None), P("ep", None, None),
        ),
        out_specs=(P("ep", None), P("ep", None, None, None)),
        check_vma=False,
    )
```

```python
import numpy as np

import jax
import jax.numpy as jnp
from jax import lax
from jax.experimental import pallas as pl
from jax.experimental.pallas import tpu as pltpu
from jax.sharding import PartitionSpec as P

MESH = pl.DeviceIdType.MESH
F32 = jnp.float32
BF16 = jnp.bfloat16
GROUP_SIZE = 32
PLANES = 4
EARLY = 2
STATE_BLOCK = 8
epsilon = 1e-06


FAR = (2, 1, 3, 0)


def digits(me):
    return me // 32, (me // 8) % 4, (me // 2) % 4, me % 2


def hops(plane, i):
    t, u = i // 8, (i % 8) // 2
    steps = [FAR[(plane + 2 - t - u) % 4], FAR[t], FAR[u]]
    return sum(min(step, 4 - step) for step in steps)


def chunk_order(plane):
    return list(range(31 if plane == PLANES - 1 else 32))


def each_partner(me, sign, plane, action, order=None):
    z, y, x, c = digits(me)
    planes = [((z + 4 + sign * far) % 4) * 32 for far in FAR]
    lines = [((y + 4 + sign * far) % 4) * 8 for far in FAR]
    inner = [
        ((x + 4 + sign * FAR[i // 2]) % 4) * 2 + (c + 1 - i % 2) % 2 for i in range(8)
    ]
    for p, i in order or [(plane, i) for i in chunk_order(plane)]:
        t = i // 8
        offset = (p + 2 - t - (i % 8) // 2) % 4
        action(p * 32 + i, planes[offset] + lines[t] + inner[i % 8])


def slot_experts(me, r):
    z, y, x, c = digits(me)
    j = r >> 1

    def far(t):
        return (2 + 3 * ((t * (t + 1)) >> 1)) & 3

    return (
        ((z + far(((j >> 5) + 2 - (j >> 3) - (j >> 1)) & 3)) & 3) * 32
        + ((y + far((j >> 3) & 3)) & 3) * 8
        + ((x + far((j >> 1) & 3)) & 3) * 2
        + ((c + 1 - (j & 1)) & 1)
    )


def rms_scale(values, gains):
    return values * lax.rsqrt(jnp.mean(values * values, axis=-1, keepdims=True) + epsilon) * gains


def layer_kernel(
    tokens_hbm, places_hbm, norm_gain_hbm, query_hbm, key_hbm, value_hbm, gating_hbm, decay_hbm,
    state_hbm, head_gain_hbm, out_hbm, moe_gain_hbm, route_hbm, group_hbm, inner_hbm, gate_hbm,
    up_hbm, down_hbm, inverse_hbm,
    out_ref, state,
    tokens, places, norm_gain, decay, head_gain, moe_gain, route, group, inner, inverse,
    w_query, w_key, w_value, w_gating, w_out, w_gate, w_up, w_down,
    keys_t, queries, values_h, decay_h, reading,
    token_out, token_in, mixed_out, mixed_in, results, returned,
    small_sems, weight_sems, state_sems,
    send_tok, recv_tok, send_mix, recv_mix, send_res, recv_res,
):
    me = lax.axis_index("ep")
    rows, width = tokens.shape
    heads, head_width = values_h.shape[1:]
    n = token_out.shape[0]
    slots = 2 * n
    per = n // PLANES
    early = EARLY * per
    blocks = rows // STATE_BLOCK

    def start(source, target, sem):
        copy = pltpu.make_async_copy(source, target, sem)
        copy.start()
        return copy

    smalls = [
        start(s, t, small_sems.at[i])
        for i, (s, t) in enumerate(
            (
                (group_hbm, group), (inner_hbm, inner), (tokens_hbm, tokens),
                (norm_gain_hbm, norm_gain), (places_hbm, places), (inverse_hbm, inverse),
                (decay_hbm, decay), (head_gain_hbm, head_gain), (moe_gain_hbm, moe_gain),
                (route_hbm, route),
            )
        )
    ]
    barrier = pltpu.get_barrier_semaphore()

    def greet(slot, device):
        pl.semaphore_signal(barrier, inc=1, device_id=(device,), device_id_type=MESH)

    everyone = [(p, i) for p in range(PLANES) for i in chunk_order(p)]
    each_partner(me, 1, 0, greet, sorted(everyone, key=lambda pair: -hops(*pair)))
    weights = [
        start(s, t, weight_sems.at[i])
        for i, (s, t) in enumerate(
            ((key_hbm, w_key), (query_hbm, w_query), (value_hbm, w_value), (gating_hbm, w_gating))
        )
    ]
    for copy in smalls:
        copy.wait()

    first_row = group[...] * GROUP_SIZE + inner[0:1, :]
    second_row = group[...] * GROUP_SIZE + inner[1:2, :]
    sub = lax.broadcasted_iota(jnp.int32, (rows, rows), 0)
    lane = lax.broadcasted_iota(jnp.int32, (rows, rows), 1)

    def column(row):
        return jnp.sum(jnp.where(sub == lane, row, jnp.zeros_like(row)), axis=1, keepdims=True)

    first_col, second_col = column(first_row), column(second_row)

    def rank(ids_row):
        same = (first_col == ids_row).astype(F32) + (second_col == ids_row).astype(F32)
        return jnp.sum(jnp.where(sub < lane, same, 0.0), axis=0, keepdims=True)

    first_rank, second_rank = rank(first_row), rank(second_row)
    r_col = lax.broadcasted_iota(jnp.int32, (slots, 1), 0)
    expert_col = slot_experts(me, r_col)
    k_col = (r_col & 1).astype(F32)
    place = ((expert_col == first_row) & (k_col == first_rank)) | (
        (expert_col == second_row) & (k_col == second_rank)
    )
    place = place.astype(F32).astype(BF16)

    def slab(chosen, values):
        taken = jnp.dot(chosen, values, preferred_element_type=F32).astype(BF16)
        return taken.reshape(chosen.shape[0] // 2, 2, values.shape[1])

    token_out[pl.ds(0, early)] = slab(place[: 2 * early], tokens[...])
    loads = [
        start(
            state_hbm.at[pl.ds(i * STATE_BLOCK, STATE_BLOCK)],
            state.at[pl.ds(i * STATE_BLOCK, STATE_BLOCK)],
            state_sems.at[i],
        )
        for i in range(blocks)
    ]
    weights += [
        start(s, t, weight_sems.at[4 + i])
        for i, (s, t) in enumerate(
            (
                (out_hbm, w_out), (gate_hbm.at[0], w_gate), (up_hbm.at[0], w_up),
                (down_hbm.at[0], w_down),
            )
        )
    ]
    inputs = tokens[...].astype(F32)
    normed = rms_scale(inputs, norm_gain[...]).astype(BF16)
    angles = column(places[...].astype(F32)) * inverse[...]
    cosine = jnp.concatenate([jnp.cos(angles)] * 4, axis=1)
    sine = jnp.concatenate([jnp.sin(angles)] * 4, axis=1)

    def remote(source, target, send_sem, recv_sems):
        def action(slot, device):
            pltpu.make_async_remote_copy(
                src_ref=source.at[slot], dst_ref=target.at[slot], send_sem=send_sem,
                recv_sem=recv_sems, device_id=(device,), device_id_type=MESH,
            ).start()

        return action


    def project(index, weight):
        weights[index].wait()
        return jnp.dot(normed, weight[...], preferred_element_type=F32).astype(BF16).astype(F32)

    first_half = (lax.broadcasted_iota(jnp.int32, (1, heads * head_width), 1) % head_width) < (
        head_width // 2
    )

    def rotate(x):
        total = heads * head_width
        half = head_width // 2
        swapped = jnp.where(first_half, -pltpu.roll(x, total - half, 1), pltpu.roll(x, half, 1))
        return x * cosine + swapped * sine

    def transposed(x):
        pad = jnp.zeros((128 - rows, x.shape[1]), F32)
        return jnp.concatenate([x, pad], axis=0).T

    keys_t[...] = transposed(rotate(project(0, w_key)) * head_width ** (-0.5))
    query = rotate(project(1, w_query))
    query_high = query.astype(BF16).astype(F32)
    head_of = lax.broadcasted_iota(jnp.int32, (1, heads, heads * head_width), 2) // head_width
    head_row = lax.broadcasted_iota(jnp.int32, (1, heads, heads * head_width), 1)
    for i, piece in enumerate((query_high, query - query_high)):
        queries[:, pl.ds(i * heads, heads)] = jnp.where(
            head_of == head_row, piece[:, None, :], 0.0
        ).astype(BF16)
    values_h[...] = project(2, w_value).reshape(rows, heads, head_width)
    gating = project(3, w_gating)
    retain = jnp.exp(-decay[...])
    decay_h[...] = jnp.concatenate(
        [jnp.broadcast_to(retain[:, h : h + 1], (1, head_width)) for h in range(heads)], axis=0
    )

    def sequence(s, carry):
        index = jnp.full((head_width, 128), s, jnp.int32)
        rounded = []
        for h in range(heads):
            key = jnp.take_along_axis(
                keys_t[pl.ds(h * head_width, head_width)], index, axis=1, mode="promise_in_bounds"
            )[:, :head_width]
            new = decay_h[h : h + 1] * state[s, h] + key * values_h[s, h : h + 1]
            state[s, h] = new
            rounded.append(new.astype(BF16))
        read = jnp.dot(
            queries[s], jnp.concatenate(rounded, axis=0), preferred_element_type=F32
        )
        reading[s] = read[:heads] + read[heads:]
        return carry

    pl.semaphore_wait(barrier, n - 1)
    for plane in range(EARLY):
        each_partner(me, 1, plane, remote(token_out, token_in, send_tok, recv_tok.at[plane]))

    for i in range(blocks):
        loads[i].wait()
        lax.fori_loop(
            i * STATE_BLOCK, (i + 1) * STATE_BLOCK, sequence, 0, unroll=STATE_BLOCK
        )

    read = reading[...]
    read = read * lax.rsqrt(jnp.mean(read * read, axis=-1, keepdims=True) + epsilon)
    read = read.reshape(rows, heads * head_width) * head_gain[...]
    mixed = (read * (gating * jax.nn.sigmoid(gating))).astype(BF16)
    mixed_out[pl.ds(0, early)] = slab(place[: 2 * early], mixed)
    for plane in range(EARLY):
        each_partner(me, 1, plane, remote(mixed_out, mixed_in, send_mix, recv_mix.at[plane]))
    weights[4].wait()

    def mix(rows_in, mixed_rows):
        added = jnp.dot(mixed_rows, w_out[...], preferred_element_type=F32)
        return (rows_in.astype(F32) + added).astype(BF16).astype(F32)

    own_tokens = mix(tokens[...], mixed)
    direct = rms_scale(own_tokens, moe_gain[...]).astype(BF16)
    token_out[pl.ds(early, n - early)] = slab(place[2 * early :], direct)
    for plane in range(EARLY, PLANES):
        each_partner(me, 1, plane, remote(token_out, token_in, send_tok, recv_tok.at[plane]))
    token_in[n - 1] = token_out[n - 1]
    for copy in weights[5:]:
        copy.wait()

    r_row = lax.broadcasted_iota(jnp.int32, (1, slots), 1)
    expert_row = slot_experts(me, r_row)
    k_row = (r_row & 1).astype(F32)
    route_one, route_two = column(route[0:1, :]), column(route[1:2, :])
    first_k, second_k = column(first_rank), column(second_rank)
    scale = jnp.where(
        (first_col == expert_row) & (first_k == k_row), route_one, 0.0
    ) + jnp.where((second_col == expert_row) & (second_k == k_row), route_two, 0.0)
    high = scale.astype(BF16)
    low = (scale - high.astype(F32)).astype(BF16)

    def wait_block(ref, sem, begin, count):
        block = ref.at[pl.ds(begin, count)]
        pltpu.make_async_copy(block, block, sem).wait()

    for plane in range(PLANES):
        begin = plane * per
        count = per if plane < PLANES - 1 else per - 1
        wait_block(token_in, recv_tok.at[plane], begin, count)
        x = token_in[pl.ds(begin, per)].reshape(2 * per, width)
        if plane < EARLY:
            wait_block(mixed_in, recv_mix.at[plane], begin, count)
            x = mix(x, mixed_in[pl.ds(begin, per)].reshape(2 * per, mixed.shape[1]))
            x = rms_scale(x, moe_gain[...]).astype(BF16)
        gate_part = jnp.dot(x, w_gate[...], preferred_element_type=F32)
        up_part = jnp.dot(x, w_up[...], preferred_element_type=F32)
        hidden = (gate_part * jax.nn.sigmoid(gate_part) * up_part).astype(BF16)
        y = jnp.dot(hidden, w_down[...], preferred_element_type=F32).astype(BF16)
        results[pl.ds(begin, per)] = y.reshape(per, 2, width)
        each_partner(me, -1, plane, remote(results, returned, send_res, recv_res))
    returned[n - 1] = results[n - 1]

    wait_block(returned, recv_res, 0, n - 1)
    back = returned[...].reshape(slots, width)
    routed = jnp.dot(high, back, preferred_element_type=F32) + jnp.dot(
        low, back, preferred_element_type=F32
    )
    out_ref[...] = (own_tokens + routed).astype(BF16)
    wait_block(token_out, send_tok, 0, n - 1)
    wait_block(mixed_out, send_mix, 0, early)
    wait_block(results, send_res, 0, n - 1)


def write_kernel(output, new_state, output_hbm, state_hbm, sems):
    pieces = sems.shape[0] - 1
    size = new_state.shape[0] // pieces
    copies = [
        pltpu.make_async_copy(
            new_state.at[pl.ds(i * size, size)], state_hbm.at[pl.ds(i * size, size)], sems.at[i]
        )
        for i in range(pieces)
    ]
    copies.append(pltpu.make_async_copy(output, output_hbm, sems.at[pieces]))
    for copy in copies:
        copy.start()
    for copy in copies:
        copy.wait()


def local(
    tokens, history_length, norm_gain, w_query, w_key, w_value, w_gate, decay_rate, state,
    head_gain, w_out, moe_gain, route_weights, expert_group, expert_inner, expert_gate,
    expert_up, expert_down,
):
    n = lax.axis_size("ep")
    rows, width = tokens.shape
    heads, head_width = state.shape[1], state.shape[2]
    ret_width = w_query.shape[1]
    hidden = expert_gate.shape[2]
    half = head_width // 2
    inverse = 10000.0 ** (-(np.arange(128) % half).astype(np.float64) / half)
    inverse = jnp.asarray(inverse.astype(np.float32)[None])
    operands = (
        tokens, history_length.reshape(1, rows), norm_gain.reshape(1, width), w_query, w_key,
        w_value, w_gate, decay_rate.reshape(1, heads), state, head_gain.reshape(1, ret_width),
        w_out, moe_gain.reshape(1, width), route_weights.T, expert_group.reshape(1, rows),
        expert_inner.T, expert_gate, expert_up, expert_down, inverse,
    )
    vmem = pl.BlockSpec(memory_space=pltpu.VMEM)
    hbm = pl.BlockSpec(memory_space=pltpu.HBM)
    V = pltpu.VMEM
    DMA = pltpu.SemaphoreType.DMA
    output, new_state = pl.pallas_call(
        layer_kernel,
        out_shape=(V((rows, width), BF16), V(state.shape, F32)),
        in_specs=[hbm] * len(operands),
        out_specs=(vmem, vmem),
        scratch_shapes=[
            V((rows, width), BF16), V((1, rows), jnp.int32), V((1, width), F32),
            V((1, heads), F32), V((1, ret_width), F32), V((1, width), F32),
            V((2, rows), F32), V((1, rows), jnp.int32), V((2, rows), jnp.int32), V((1, 128), F32),
            V((width, ret_width), BF16), V((width, ret_width), BF16),
            V((width, ret_width), BF16), V((width, ret_width), BF16),
            V((ret_width, width), BF16), V((width, hidden), BF16), V((width, hidden), BF16),
            V((hidden, width), BF16),
            V((ret_width, 128), F32), V((rows, 2 * heads, ret_width), BF16),
            V((rows, heads, head_width), F32),
            V((heads, head_width), F32), V((rows, heads, head_width), F32),
            V((n, 2, width), BF16), V((n, 2, width), BF16),
            V((n, 2, ret_width), BF16), V((n, 2, ret_width), BF16),
            V((n, 2, width), BF16), V((n, 2, width), BF16),
            DMA((10,)), DMA((8,)), DMA((rows // STATE_BLOCK,)),
            DMA, DMA((PLANES,)), DMA, DMA((EARLY,)), DMA, DMA,
        ],
        compiler_params=pltpu.CompilerParams(
            collective_id=0, has_side_effects=True, vmem_limit_bytes=46 * 1024 * 1024
        ),
    )(*operands)
    pieces = 8
    return pl.pallas_call(
        write_kernel,
        out_shape=(
            jax.ShapeDtypeStruct((rows, width), BF16), jax.ShapeDtypeStruct(state.shape, F32),
        ),
        in_specs=[vmem, vmem],
        out_specs=(hbm, hbm),
        scratch_shapes=[DMA((pieces + 1,))],
        compiler_params=pltpu.CompilerParams(vmem_limit_bytes=1024 * 1024),
    )(
        pltpu.with_memory_space_constraint(output, pltpu.VMEM),
        pltpu.with_memory_space_constraint(new_state, pltpu.VMEM),
    )


def solution(mesh):
    return jax.shard_map(
        local,
        mesh=mesh,
        in_specs=(
            P("ep", None), P("ep"), P(), P(), P(), P(), P(), P(), P("ep", None, None, None),
            P(), P(), P(), P("ep", None), P("ep"), P("ep", None), P("ep", None, None),
            P("ep", None, None), P("ep", None, None),
        ),
        out_specs=(P("ep", None), P("ep", None, None, None)),
        check_vma=False,
    )
```

```python
import numpy as np

import jax
import jax.numpy as jnp
from jax import lax
from jax.experimental import pallas as pl
from jax.experimental.pallas import tpu as pltpu
from jax.sharding import PartitionSpec as P

MESH = pl.DeviceIdType.MESH
F32 = jnp.float32
BF16 = jnp.bfloat16
GROUP_SIZE = 32
PLANES = 4
EARLY = 2
STATE_BLOCK = 8
epsilon = 1e-06


FAR = (2, 1, 3, 0)


def digits(me):
    return me // 32, (me // 8) % 4, (me // 2) % 4, me % 2


def hops(plane, i):
    t, u = i // 8, (i % 8) // 2
    steps = [FAR[(plane + 2 - t - u) % 4], FAR[t], FAR[u]]
    return sum(min(step, 4 - step) for step in steps)


def chunk_order(plane):
    return list(range(31 if plane == PLANES - 1 else 32))


def each_partner(me, sign, plane, action, order=None):
    z, y, x, c = digits(me)
    planes = [((z + 4 + sign * far) % 4) * 32 for far in FAR]
    lines = [((y + 4 + sign * far) % 4) * 8 for far in FAR]
    inner = [
        ((x + 4 + sign * FAR[i // 2]) % 4) * 2 + (c + 1 - i % 2) % 2 for i in range(8)
    ]
    for p, i in order or [(plane, i) for i in chunk_order(plane)]:
        t = i // 8
        offset = (p + 2 - t - (i % 8) // 2) % 4
        action(p * 32 + i, planes[offset] + lines[t] + inner[i % 8])


def slot_experts(me, r):
    z, y, x, c = digits(me)
    j = r >> 1

    def far(t):
        return (2 + 3 * ((t * (t + 1)) >> 1)) & 3

    return (
        ((z + far(((j >> 5) + 2 - (j >> 3) - (j >> 1)) & 3)) & 3) * 32
        + ((y + far((j >> 3) & 3)) & 3) * 8
        + ((x + far((j >> 1) & 3)) & 3) * 2
        + ((c + 1 - (j & 1)) & 1)
    )


def rms_scale(values, gains):
    return values * lax.rsqrt(jnp.mean(values * values, axis=-1, keepdims=True) + epsilon) * gains


def layer_kernel(
    tokens_hbm, places_hbm, norm_gain_hbm, query_hbm, key_hbm, value_hbm, gating_hbm, decay_hbm,
    state_hbm, head_gain_hbm, out_hbm, moe_gain_hbm, route_hbm, group_hbm, inner_hbm, gate_hbm,
    up_hbm, down_hbm, inverse_hbm,
    out_ref, state,
    tokens, places, norm_gain, decay, head_gain, moe_gain, route, group, inner, inverse,
    w_query, w_key, w_value, w_gating, w_out, w_gate, w_up, w_down,
    keys_t, queries, values_h, decay_h, reading,
    token_out, token_in, mixed_out, mixed_in, results, returned,
    small_sems, weight_sems, state_sems,
    send_tok, recv_tok, send_mix, recv_mix, send_res, recv_res,
):
    me = lax.axis_index("ep")
    rows, width = tokens.shape
    heads, head_width = values_h.shape[1:]
    n = token_out.shape[0]
    slots = 2 * n
    per = n // PLANES
    early = EARLY * per
    blocks = rows // STATE_BLOCK

    def start(source, target, sem):
        copy = pltpu.make_async_copy(source, target, sem)
        copy.start()
        return copy

    smalls = [
        start(s, t, small_sems.at[i])
        for i, (s, t) in enumerate(
            (
                (group_hbm, group), (inner_hbm, inner), (tokens_hbm, tokens),
                (norm_gain_hbm, norm_gain), (places_hbm, places), (inverse_hbm, inverse),
                (decay_hbm, decay), (head_gain_hbm, head_gain), (moe_gain_hbm, moe_gain),
                (route_hbm, route),
            )
        )
    ]
    barrier = pltpu.get_barrier_semaphore()

    def greet(slot, device):
        pl.semaphore_signal(barrier, inc=1, device_id=(device,), device_id_type=MESH)

    everyone = [(p, i) for p in range(PLANES) for i in chunk_order(p)]
    each_partner(me, 1, 0, greet, sorted(everyone, key=lambda pair: -hops(*pair)))
    weights = [
        start(s, t, weight_sems.at[i])
        for i, (s, t) in enumerate(
            ((key_hbm, w_key), (query_hbm, w_query), (value_hbm, w_value), (gating_hbm, w_gating))
        )
    ]
    for copy in smalls:
        copy.wait()

    first_row = group[...] * GROUP_SIZE + inner[0:1, :]
    second_row = group[...] * GROUP_SIZE + inner[1:2, :]
    sub = lax.broadcasted_iota(jnp.int32, (rows, rows), 0)
    lane = lax.broadcasted_iota(jnp.int32, (rows, rows), 1)

    def column(row):
        return jnp.sum(jnp.where(sub == lane, row, jnp.zeros_like(row)), axis=1, keepdims=True)

    first_col, second_col = column(first_row), column(second_row)

    def rank(ids_row):
        same = (first_col == ids_row).astype(F32) + (second_col == ids_row).astype(F32)
        return jnp.sum(jnp.where(sub < lane, same, 0.0), axis=0, keepdims=True)

    first_rank, second_rank = rank(first_row), rank(second_row)
    r_col = lax.broadcasted_iota(jnp.int32, (slots, 1), 0)
    expert_col = slot_experts(me, r_col)
    k_col = (r_col & 1).astype(F32)
    place = ((expert_col == first_row) & (k_col == first_rank)) | (
        (expert_col == second_row) & (k_col == second_rank)
    )
    place = place.astype(F32).astype(BF16)

    def slab(chosen, values):
        taken = jnp.dot(chosen, values, preferred_element_type=F32).astype(BF16)
        return taken.reshape(chosen.shape[0] // 2, 2, values.shape[1])

    token_out[pl.ds(0, early)] = slab(place[: 2 * early], tokens[...])
    loads = [
        start(
            state_hbm.at[pl.ds(i * STATE_BLOCK, STATE_BLOCK)],
            state.at[pl.ds(i * STATE_BLOCK, STATE_BLOCK)],
            state_sems.at[i],
        )
        for i in range(blocks)
    ]
    weights += [
        start(s, t, weight_sems.at[4 + i])
        for i, (s, t) in enumerate(
            (
                (out_hbm, w_out), (gate_hbm.at[0], w_gate), (up_hbm.at[0], w_up),
                (down_hbm.at[0], w_down),
            )
        )
    ]
    inputs = tokens[...].astype(F32)
    normed = rms_scale(inputs, norm_gain[...]).astype(BF16)
    angles = column(places[...].astype(F32)) * inverse[...]
    cosine = jnp.concatenate([jnp.cos(angles)] * 4, axis=1)
    sine = jnp.concatenate([jnp.sin(angles)] * 4, axis=1)

    def remote(source, target, send_sem, recv_sems):
        def action(slot, device):
            pltpu.make_async_remote_copy(
                src_ref=source.at[slot], dst_ref=target.at[slot], send_sem=send_sem,
                recv_sem=recv_sems, device_id=(device,), device_id_type=MESH,
            ).start()

        return action


    def project(index, weight):
        weights[index].wait()
        return jnp.dot(normed, weight[...], preferred_element_type=F32).astype(BF16).astype(F32)

    first_half = (lax.broadcasted_iota(jnp.int32, (1, heads * head_width), 1) % head_width) < (
        head_width // 2
    )

    def rotate(x):
        total = heads * head_width
        half = head_width // 2
        swapped = jnp.where(first_half, -pltpu.roll(x, total - half, 1), pltpu.roll(x, half, 1))
        return x * cosine + swapped * sine

    def transposed(x):
        pad = jnp.zeros((128 - rows, x.shape[1]), F32)
        return jnp.concatenate([x, pad], axis=0).T

    keys_t[...] = transposed(rotate(project(0, w_key)) * head_width ** (-0.5))
    query = rotate(project(1, w_query))
    query_high = query.astype(BF16).astype(F32)
    head_of = lax.broadcasted_iota(jnp.int32, (1, heads, heads * head_width), 2) // head_width
    head_row = lax.broadcasted_iota(jnp.int32, (1, heads, heads * head_width), 1)
    for i, piece in enumerate((query_high, query - query_high)):
        queries[:, pl.ds(i * heads, heads)] = jnp.where(
            head_of == head_row, piece[:, None, :], 0.0
        ).astype(BF16)
    values_h[...] = project(2, w_value).reshape(rows, heads, head_width)
    gating = project(3, w_gating)
    retain = jnp.exp(-decay[...])
    decay_h[...] = jnp.concatenate(
        [jnp.broadcast_to(retain[:, h : h + 1], (1, head_width)) for h in range(heads)], axis=0
    )

    def sequence(s, carry):
        index = jnp.full((head_width, 128), s, jnp.int32)
        rounded = []
        for h in range(heads):
            key = jnp.take_along_axis(
                keys_t[pl.ds(h * head_width, head_width)], index, axis=1, mode="promise_in_bounds"
            )[:, :head_width]
            new = decay_h[h : h + 1] * state[s, h] + key * values_h[s, h : h + 1]
            state[s, h] = new
            rounded.append(new.astype(BF16))
        read = jnp.dot(
            queries[s], jnp.concatenate(rounded, axis=0), preferred_element_type=F32
        )
        reading[s] = read[:heads] + read[heads:]
        return carry

    pl.semaphore_wait(barrier, n - 1)
    for plane in range(EARLY):
        each_partner(me, 1, plane, remote(token_out, token_in, send_tok, recv_tok.at[plane]))

    for i in range(blocks):
        loads[i].wait()
        lax.fori_loop(
            i * STATE_BLOCK, (i + 1) * STATE_BLOCK, sequence, 0, unroll=STATE_BLOCK
        )

    read = reading[...]
    read = read * lax.rsqrt(jnp.mean(read * read, axis=-1, keepdims=True) + epsilon)
    read = read.reshape(rows, heads * head_width) * head_gain[...]
    mixed = (read * (gating * jax.nn.sigmoid(gating))).astype(BF16)
    mixed_out[pl.ds(0, early)] = slab(place[: 2 * early], mixed)
    for plane in range(EARLY):
        each_partner(me, 1, plane, remote(mixed_out, mixed_in, send_mix, recv_mix.at[plane]))
    weights[4].wait()

    def mix(rows_in, mixed_rows):
        added = jnp.dot(mixed_rows, w_out[...], preferred_element_type=F32)
        return (rows_in.astype(F32) + added).astype(BF16).astype(F32)

    own_tokens = mix(tokens[...], mixed)
    direct = rms_scale(own_tokens, moe_gain[...]).astype(BF16)
    token_out[pl.ds(early, n - early)] = slab(place[2 * early :], direct)
    for plane in range(EARLY, PLANES):
        each_partner(me, 1, plane, remote(token_out, token_in, send_tok, recv_tok.at[plane]))
    token_in[n - 1] = token_out[n - 1]
    for copy in weights[5:]:
        copy.wait()

    r_row = lax.broadcasted_iota(jnp.int32, (1, slots), 1)
    expert_row = slot_experts(me, r_row)
    k_row = (r_row & 1).astype(F32)
    route_one, route_two = column(route[0:1, :]), column(route[1:2, :])
    first_k, second_k = column(first_rank), column(second_rank)
    scale = jnp.where(
        (first_col == expert_row) & (first_k == k_row), route_one, 0.0
    ) + jnp.where((second_col == expert_row) & (second_k == k_row), route_two, 0.0)
    high = scale.astype(BF16)
    low = (scale - high.astype(F32)).astype(BF16)

    def wait_block(ref, sem, begin, count):
        block = ref.at[pl.ds(begin, count)]
        pltpu.make_async_copy(block, block, sem).wait()

    for plane in range(PLANES):
        begin = plane * per
        count = per if plane < PLANES - 1 else per - 1
        wait_block(token_in, recv_tok.at[plane], begin, count)
        x = token_in[pl.ds(begin, per)].reshape(2 * per, width)
        if plane < EARLY:
            wait_block(mixed_in, recv_mix.at[plane], begin, count)
            x = mix(x, mixed_in[pl.ds(begin, per)].reshape(2 * per, mixed.shape[1]))
            x = rms_scale(x, moe_gain[...]).astype(BF16)
        gate_part = jnp.dot(x, w_gate[...], preferred_element_type=F32)
        up_part = jnp.dot(x, w_up[...], preferred_element_type=F32)
        hidden = (gate_part * jax.nn.sigmoid(gate_part) * up_part).astype(BF16)
        y = jnp.dot(hidden, w_down[...], preferred_element_type=F32).astype(BF16)
        results[pl.ds(begin, per)] = y.reshape(per, 2, width)
        each_partner(me, -1, plane, remote(results, returned, send_res, recv_res.at[plane]))
    returned[n - 1] = results[n - 1]

    both = jnp.concatenate([high, low], axis=0)
    routed = own_tokens
    for plane in range(PLANES):
        begin = plane * per
        wait_block(returned, recv_res.at[plane], begin, per if plane < PLANES - 1 else per - 1)
        back = returned[pl.ds(begin, per)].reshape(2 * per, width)
        parts = jnp.dot(
            both[:, 2 * begin : 2 * (begin + per)], back, preferred_element_type=F32
        )
        routed = routed + parts[:rows] + parts[rows:]
    out_ref[...] = routed.astype(BF16)
    wait_block(token_out, send_tok, 0, n - 1)
    wait_block(mixed_out, send_mix, 0, early)
    wait_block(results, send_res, 0, n - 1)


def write_kernel(output, new_state, output_hbm, state_hbm, sems):
    pieces = sems.shape[0] - 1
    size = new_state.shape[0] // pieces
    copies = [
        pltpu.make_async_copy(
            new_state.at[pl.ds(i * size, size)], state_hbm.at[pl.ds(i * size, size)], sems.at[i]
        )
        for i in range(pieces)
    ]
    copies.append(pltpu.make_async_copy(output, output_hbm, sems.at[pieces]))
    for copy in copies:
        copy.start()
    for copy in copies:
        copy.wait()


def local(
    tokens, history_length, norm_gain, w_query, w_key, w_value, w_gate, decay_rate, state,
    head_gain, w_out, moe_gain, route_weights, expert_group, expert_inner, expert_gate,
    expert_up, expert_down,
):
    n = lax.axis_size("ep")
    rows, width = tokens.shape
    heads, head_width = state.shape[1], state.shape[2]
    ret_width = w_query.shape[1]
    hidden = expert_gate.shape[2]
    half = head_width // 2
    inverse = 10000.0 ** (-(np.arange(128) % half).astype(np.float64) / half)
    inverse = jnp.asarray(inverse.astype(np.float32)[None])
    operands = (
        tokens, history_length.reshape(1, rows), norm_gain.reshape(1, width), w_query, w_key,
        w_value, w_gate, decay_rate.reshape(1, heads), state, head_gain.reshape(1, ret_width),
        w_out, moe_gain.reshape(1, width), route_weights.T, expert_group.reshape(1, rows),
        expert_inner.T, expert_gate, expert_up, expert_down, inverse,
    )
    vmem = pl.BlockSpec(memory_space=pltpu.VMEM)
    hbm = pl.BlockSpec(memory_space=pltpu.HBM)
    V = pltpu.VMEM
    DMA = pltpu.SemaphoreType.DMA
    output, new_state = pl.pallas_call(
        layer_kernel,
        out_shape=(V((rows, width), BF16), V(state.shape, F32)),
        in_specs=[hbm] * len(operands),
        out_specs=(vmem, vmem),
        scratch_shapes=[
            V((rows, width), BF16), V((1, rows), jnp.int32), V((1, width), F32),
            V((1, heads), F32), V((1, ret_width), F32), V((1, width), F32),
            V((2, rows), F32), V((1, rows), jnp.int32), V((2, rows), jnp.int32), V((1, 128), F32),
            V((width, ret_width), BF16), V((width, ret_width), BF16),
            V((width, ret_width), BF16), V((width, ret_width), BF16),
            V((ret_width, width), BF16), V((width, hidden), BF16), V((width, hidden), BF16),
            V((hidden, width), BF16),
            V((ret_width, 128), F32), V((rows, 2 * heads, ret_width), BF16),
            V((rows, heads, head_width), F32),
            V((heads, head_width), F32), V((rows, heads, head_width), F32),
            V((n, 2, width), BF16), V((n, 2, width), BF16),
            V((n, 2, ret_width), BF16), V((n, 2, ret_width), BF16),
            V((n, 2, width), BF16), V((n, 2, width), BF16),
            DMA((10,)), DMA((8,)), DMA((rows // STATE_BLOCK,)),
            DMA, DMA((PLANES,)), DMA, DMA((EARLY,)), DMA, DMA((PLANES,)),
        ],
        compiler_params=pltpu.CompilerParams(
            collective_id=0, has_side_effects=True, vmem_limit_bytes=46 * 1024 * 1024
        ),
    )(*operands)
    pieces = 8
    return pl.pallas_call(
        write_kernel,
        out_shape=(
            jax.ShapeDtypeStruct((rows, width), BF16), jax.ShapeDtypeStruct(state.shape, F32),
        ),
        in_specs=[vmem, vmem],
        out_specs=(hbm, hbm),
        scratch_shapes=[DMA((pieces + 1,))],
        compiler_params=pltpu.CompilerParams(vmem_limit_bytes=1024 * 1024),
    )(
        pltpu.with_memory_space_constraint(output, pltpu.VMEM),
        pltpu.with_memory_space_constraint(new_state, pltpu.VMEM),
    )


def solution(mesh):
    return jax.shard_map(
        local,
        mesh=mesh,
        in_specs=(
            P("ep", None), P("ep"), P(), P(), P(), P(), P(), P(), P("ep", None, None, None),
            P(), P(), P(), P("ep", None), P("ep"), P("ep", None), P("ep", None, None),
            P("ep", None, None), P("ep", None, None),
        ),
        out_specs=(P("ep", None), P("ep", None, None, None)),
        check_vma=False,
    )
```
